512 devices in a mesh: grp: 2 (over y), sp: 16 (over z), tp: 16 (over x, core).
Axes of the slice: x: 8, y: 2, z: 16, core: 2. Of those that a mesh axis runs over, the one named last changes fastest.
The devices are a block of a 8x16x16 slice.
Arguments:
- tokens: bfloat16 [8192, 2048], P(('grp', 'sp'), 'tp'), parts along dimension 0, may hold values from -40 to 40
- norm_gain: float32 [2, 2048], replicated, may hold values from 0.1 to 1.9
- value_proj: bfloat16 [2, 1024, 2048], P(None, 'tp', 'sp'), may hold values from -0.125 to 0.125
- gate_proj: bfloat16 [2, 1024, 2048], P(None, 'tp', 'sp'), may hold values from -0.125 to 0.125
- conv_taps: float32 [2, 4, 1024], P(None, None, 'tp'), may hold values from -3 to 3
- recur_map: bfloat16 [2, 16, 64, 64], P(None, 'tp'), may hold values from -0.75 to 0.75
- input_map: bfloat16 [2, 16, 64, 64], P(None, 'tp'), may hold values from -0.75 to 0.75
- decay_param: float32 [2, 1024], P(None, 'tp'), may hold values from 3 to 16
- decay_offset: float32 [2, 1024, 4096], P(None, 'tp', 'sp'), may hold values from -3 to 0
- mix_proj: bfloat16 [2, 1024, 2048], P(None, 'sp', 'tp'), may hold values from -0.1875 to 0.1875
Outputs:
- mixed_out: bfloat16 [8192, 2048], P(('grp', 'sp'), 'tp'), parts along dimension 0
The draws below stay inside these ranges and needn't reach their ends.
There are 2 independent parts, one for each index of `grp`. The reference program is written for one: setup_inputs(seed, part) draws one part's arguments, and reference() takes and returns one part's arrays. A program takes and returns all parts, laid end to end along the dimension named above; an argument that names none is the same for every part. Nothing has to cross between parts.
All inputs are finite; a program needn't handle non-finite values.
Results may differ from the reference program's by a relative error of at most 0.013.
Values may be sent and summed in bfloat16 or wider, within the bound.
No kernel may reach another device: no remote copies, remote signals or barrier semaphores. Data moves between devices by JAX's collectives and lax.ppermute only.
A program may use at most 64 MiB of HBM per device.

```python
import jax
import jax.numpy as jnp
from jax import lax

D = 2048
HEADS = 16
D_LRU = 1024
HEAD_DIM = 64
CONV = 4
LAYERS = 2
TOK_DEV = 256
LENGTH = 4096


def channel_rates(key):
    base = jax.random.fold_in(key, 11)
    keys = jax.random.split(base, 3)
    shape = (LAYERS, D // 2)
    share = 0.5
    fastest = jax.random.uniform(keys[0], shape, jnp.float32) < share
    short_span = min(30, TOK_DEV // 4) * 1.0
    long_span = min(100, TOK_DEV // 2) * 1.0
    fast_span = jnp.exp(jax.random.uniform(keys[1], shape, jnp.float32, jnp.log(short_span), jnp.log(long_span)))
    slow_rate = jnp.exp(jax.random.uniform(keys[2], shape, jnp.float32, jnp.log(0.01), jnp.log(0.04))) / LENGTH
    return jnp.where(fastest, 0.25 / fast_span, slow_rate)


def draw_decay_param(key, part):
    rates = channel_rates(key)
    return -jnp.log(jnp.expm1(rates))


def draw_decay_offset(key, part):
    rates = channel_rates(key)
    keys = jax.random.split(jax.random.fold_in(key, 23), 3)
    blocks = LENGTH // TOK_DEV
    stretch = jnp.exp(jax.random.uniform(keys[0], (LAYERS, D // 2, blocks), jnp.float32, 0.0, jnp.log(3.0)))
    stretch = jnp.repeat(stretch, TOK_DEV, axis=2)
    reference_level = -4.0 * rates[:, :, None] * (stretch - 1.0)
    slot_positions = jax.random.randint(keys[1], (LAYERS, 3), 0, LENGTH)
    share_part = jax.random.uniform(keys[2], (LAYERS, 3, D // 2), jnp.float32, 0.2, 0.5)
    match_count = (slot_positions[:, :, None] == jnp.arange(LENGTH)[None, None, :]).astype(jnp.float32)
    spike_groups = jnp.einsum('rkv,rkq->rvq', jnp.log1p(-share_part), match_count)
    return (reference_level + spike_groups).astype(jnp.float32)


def draw_tokens(key, part):
    keys = jax.random.split(key, 3)
    noise = jnp.clip(jax.random.normal(keys[0], (LENGTH, D), jnp.float32), -4.0, 4.0)
    row_scale = jnp.exp(jax.random.uniform(keys[1], (LENGTH, 1), jnp.float32, 0.0, jnp.log(10.0))) / 5.0
    column_upper = 3.0
    position = jnp.arange(D, dtype=jnp.float32)[None, :] / D
    jitter = jax.random.uniform(keys[2], (1, D), jnp.float32, -0.3, 0.3)
    column_scale = jnp.exp(jnp.log(column_upper) * position + jitter)
    return (noise * row_scale * column_scale).astype(jnp.bfloat16)


def steps_of(own_key, dims, cuts, low, top_value):
    gain = 1.0
    for dim, blocks in cuts:
        steps = jax.random.uniform(jax.random.fold_in(jax.random.fold_in(own_key, 6), dim), (blocks,), jnp.float32, low / len(cuts), top_value / len(cuts))
        gain = gain * jnp.repeat(jnp.exp(steps), dims[dim] // blocks).reshape((-1,) + (1,) * (len(dims) - 1 - dim))
    return gain


def gaussian(stream_key, dims, spread, most, shards=(), held_as=jnp.bfloat16):
    level = steps_of(stream_key, dims, shards, -0.22, 0.18) if shards else 1.0
    result = jax.random.normal(stream_key, dims, jnp.float32) * spread * level
    return jnp.minimum(jnp.maximum(result, -most), most).astype(held_as)


def setup_inputs(seed: int = 0, part: int = 0) -> dict:
    streams_of = jax.random.split(jax.random.key(seed), 11)
    own_keys = jax.random.split(jax.random.fold_in(streams_of[10], part), 11)
    return {
        "tokens": draw_tokens(jax.random.fold_in(jax.random.fold_in(streams_of[10], part), 71), part),
        "norm_gain": jnp.clip(1.0 + 0.18 * jax.random.normal(streams_of[1], (LAYERS, D), jnp.float32), 0.1, 1.9),
        "value_proj": gaussian(streams_of[2], (LAYERS, D_LRU, D), D ** -0.5, 0.125, ((1, 16), (2, 16))),
        "gate_proj": gaussian(streams_of[3], (LAYERS, D_LRU, D), D ** -0.5, 0.125, ((1, 16), (2, 16))),
        "conv_taps": gaussian(streams_of[4], (LAYERS, CONV, D_LRU), CONV ** -0.5, 3.0, ((2, 16),), jnp.float32),
        "recur_map": gaussian(streams_of[5], (LAYERS, HEADS, HEAD_DIM, HEAD_DIM), HEAD_DIM ** -0.5, 0.75, ((1, 16),)),
        "input_map": gaussian(streams_of[6], (LAYERS, HEADS, HEAD_DIM, HEAD_DIM), HEAD_DIM ** -0.5, 0.75, ((1, 16),)),
        "decay_param": draw_decay_param(jax.random.fold_in(streams_of[10], 71), part),
        "decay_offset": draw_decay_offset(jax.random.fold_in(streams_of[10], 71), part),
        "mix_proj": gaussian(streams_of[9], (LAYERS, D_LRU, D), D_LRU ** -0.5, 0.1875, ((1, 16), (2, 16))),
    }


EPS = 1e-06
RATE_SCALE = 8.0

def combine_pairs(earlier, later):
    return (earlier[0] * later[0], later[0] * earlier[1] + later[1])

def mixer_layer(residual, gain_row, value_weights, gate_weights, taps_layer, recur_layer, input_layer, param_layer, offset_layer, mix_weights):
    wide = residual.astype(jnp.float32)
    scale_factor = lax.rsqrt(lax.optimization_barrier(jnp.mean(wide * wide, axis=1)) + EPS)
    scaled = (wide * gain_row[None, :]).astype(jnp.bfloat16)
    value_rows = (jnp.dot(value_weights, scaled.T, preferred_element_type=jnp.float32) * scale_factor[None, :]).astype(jnp.bfloat16)
    gate_rows = (jnp.dot(gate_weights, scaled.T, preferred_element_type=jnp.float32) * scale_factor[None, :]).astype(jnp.bfloat16)
    padded = jnp.concatenate([jnp.zeros((D_LRU, CONV - 1), jnp.bfloat16), value_rows], axis=1)
    smoothed = jnp.zeros((D_LRU, LENGTH), jnp.float32)
    for tap_index in range(CONV):
        smoothed = smoothed + taps_layer[tap_index][:, None] * padded[:, tap_index:tap_index + LENGTH].astype(jnp.float32)
    smoothed_half = smoothed.astype(jnp.bfloat16).astype(jnp.float32).reshape(HEADS, HEAD_DIM, LENGTH)
    recur = jax.nn.sigmoid(jnp.einsum('hit,hij->hjt', smoothed_half, recur_layer.astype(jnp.float32)).reshape(D_LRU, LENGTH))
    inputs = jax.nn.sigmoid(jnp.einsum('hit,hij->hjt', smoothed_half, input_layer.astype(jnp.float32)).reshape(D_LRU, LENGTH))
    log_decay = -RATE_SCALE * recur * jax.nn.softplus(-param_layer)[:, None] + offset_layer
    decay = jnp.exp(log_decay)
    driving = jnp.sqrt(-jnp.expm1(2.0 * log_decay)) * inputs * smoothed
    _, hidden_state = lax.associative_scan(combine_pairs, (decay, driving), axis=1)
    branch = (hidden_state * jax.nn.silu(gate_rows.astype(jnp.float32))).astype(jnp.bfloat16)
    projected = jnp.dot(branch.T, mix_weights, preferred_element_type=jnp.float32)
    return (wide + projected).astype(jnp.bfloat16)

def reference(tokens, norm_gain, value_proj, gate_proj, conv_taps, recur_map, input_map, decay_param, decay_offset, mix_proj):
    residual = tokens
    for layer_index in range(LAYERS):
        residual = mixer_layer(residual, norm_gain[layer_index], value_proj[layer_index], gate_proj[layer_index], conv_taps[layer_index], recur_map[layer_index], input_map[layer_index], decay_param[layer_index], decay_offset[layer_index], mix_proj[layer_index])
    return residual
```

```python
import jax
import jax.numpy as jnp
from jax import lax
from jax.experimental import pallas as pl
from jax.experimental.pallas import tpu as pltpu
from jax.sharding import Mesh, PartitionSpec as P

LAYERS = 2
EPS = 1e-06
RATE_SCALE = 8.0
LANES = 128


def one_minus_exp(u):
    series = 1.0
    for n in range(9, 1, -1):
        series = 1.0 + u * series * (1.0 / n)
    return jnp.where(u > -0.5, -u * series, 1.0 - jnp.exp(u))


def scan_kernel(value_ref, before_ref, consts_ref, maps_ref, offset_ref, cum_ref, state_ref, msg_ref):
    channels, tok = value_ref.shape
    taps = 4
    value = value_ref[...].astype(jnp.float32)
    full = jnp.concatenate([before_ref[...].astype(jnp.float32), value], axis=1)
    smoothed = consts_ref[:, taps - 1 : taps] * value
    for back in range(1, taps):
        shifted = pltpu.roll(full, back, axis=1)[:, LANES:]
        smoothed = smoothed + consts_ref[:, taps - 1 - back : taps - back] * shifted
    half = smoothed.astype(jnp.bfloat16)
    gates = lax.dot_general(
        maps_ref[...], half, (((1,), (0,)), ((), ())), preferred_element_type=jnp.float32
    )
    gates = 1.0 / (1.0 + jnp.exp(-gates))
    recur, inputs = gates[:channels], gates[channels:]
    log_decay = consts_ref[:, taps : taps + 1] * recur + offset_ref[...]
    a = jnp.exp(log_decay)
    b = jnp.sqrt(one_minus_exp(2.0 * log_decay)) * inputs * smoothed
    lane = lax.broadcasted_iota(jnp.int32, (channels, tok), 1)
    step = 1
    while step < tok:
        inside = lane >= step
        b = jnp.where(inside, a * pltpu.roll(b, step, axis=1), 0.0) + b
        a = jnp.where(inside, pltpu.roll(a, step, axis=1), 1.0) * a
        step *= 2
    cum_ref[...] = a
    state_ref[...] = b
    last = jnp.concatenate([a[:, tok - LANES :], b[:, tok - LANES :]], axis=0)
    row = last.T[LANES - 1 : LANES, :]
    msg_ref[...] = jnp.broadcast_to(row[None], msg_ref.shape)


def close_kernel(pos_ref, msgs_ref, cum_ref, state_ref, gate_ref, out_ref):
    channels, tok = cum_ref.shape
    count = msgs_ref.shape[0]
    position = pos_ref[0]
    carry = jnp.zeros((1, channels), jnp.float32)
    for s in range(count - 1):
        line = msgs_ref[s]
        step = line[:, :channels] * carry + line[:, channels:]
        carry = jnp.where(s < position, step, carry)
    wide = jnp.broadcast_to(carry, (LANES, channels)).T
    wide = jnp.concatenate([wide] * (tok // LANES), axis=1)
    hidden = state_ref[...] + cum_ref[...] * wide
    gate = gate_ref[...].astype(jnp.float32)
    branch = (hidden * (gate / (1.0 + jnp.exp(-gate)))).astype(jnp.bfloat16)
    out_ref[...] = jnp.broadcast_to(branch[None], out_ref.shape)


def vmem(n):
    return [pl.BlockSpec(memory_space=pltpu.VMEM)] * n


def scan_call(value, before, consts, maps, offset, count):
    channels, tok = value.shape
    return pl.pallas_call(
        scan_kernel,
        out_shape=(
            jax.ShapeDtypeStruct((channels, tok), jnp.float32),
            jax.ShapeDtypeStruct((channels, tok), jnp.float32),
            jax.ShapeDtypeStruct((count, 1, 2 * channels), jnp.float32),
        ),
        in_specs=vmem(5),
        out_specs=tuple(vmem(3)),
        name="scan",
    )(value, before, consts, maps, offset)


def close_call(position, msgs, cum, state, gate, copies):
    channels, tok = cum.shape
    return pl.pallas_call(
        close_kernel,
        out_shape=jax.ShapeDtypeStruct((copies, channels, tok), jnp.bfloat16),
        in_specs=[pl.BlockSpec(memory_space=pltpu.SMEM)] + vmem(4),
        out_specs=vmem(1)[0],
        name="close",
    )(position, msgs, cum, state, gate)


def gather(array, axis):
    copies = jnp.broadcast_to(array, (lax.axis_size(axis), *array.shape))
    return exchange(copies, axis)


def exchange(copies, axis):
    return lax.all_to_all(copies, axis, split_axis=0, concat_axis=0, tiled=True)


def swap(array):
    return lax.ppermute(array, "core", [(0, 1), (1, 0)])


def local(
    tokens,
    norm_gain,
    value_proj,
    gate_proj,
    conv_taps,
    recur_map,
    input_map,
    decay_param,
    decay_offset,
    mix_proj,
):
    tok_rows, own_cols = tokens.shape
    channels = value_proj.shape[1]
    tap_total = conv_taps.shape[1]
    chips, count = lax.axis_size("x"), lax.axis_size("sp")
    core = lax.axis_index("core")
    position = lax.axis_index("sp").reshape(1)
    full_width = own_cols * chips * lax.axis_size("core")

    def by_core(array, dim):
        shape = array.shape
        array = array.reshape(*shape[:dim], chips, 2, *shape[dim + 1 :])
        own = lax.dynamic_index_in_dim(array, core, dim + 1, keepdims=False)
        other = lax.dynamic_index_in_dim(array, 1 - core, dim + 1, keepdims=False)
        return own, other

    rates = -RATE_SCALE * jax.nn.softplus(-decay_param)
    consts = jnp.concatenate([conv_taps.transpose(0, 2, 1), rates[:, :, None]], axis=2)
    consts = jnp.pad(consts, ((0, 0), (0, 0), (0, LANES - consts.shape[2])))
    maps = jnp.concatenate([recur_map[:, 0], input_map[:, 0]], axis=2).transpose(0, 2, 1)
    gains = norm_gain.reshape(LAYERS, chips * 2, own_cols)
    residual = tokens
    for layer in range(LAYERS):
        shards = jnp.concatenate([value_proj[layer], gate_proj[layer]], axis=0)
        mine = gather(residual, "x")
        weights = gather(shards, "sp")
        theirs = swap(mine)
        product, squares = 0.0, 0.0
        for piece, gain, weight in zip((mine, theirs), by_core(gains[layer], 0), by_core(weights, 0)):
            wide = piece.astype(jnp.float32)
            scaled = (wide * gain[:, None, :]).astype(jnp.bfloat16)
            product += jnp.einsum(
                "jcf,jtf->ct", weight, scaled, preferred_element_type=jnp.float32
            )
            squares += jnp.sum(wide * wide, axis=(0, 2))
        projected = (product * lax.rsqrt(squares / full_width + EPS)[None, :]).astype(jnp.bfloat16)
        value_rows, gate_rows = projected[:channels], projected[channels:]
        before = lax.ppermute(
            value_rows[:, tok_rows - LANES :], "sp", [(i, i + 1) for i in range(count - 1)]
        )
        cum, state, msg = scan_call(
            value_rows, before, consts[layer], maps[layer], decay_offset[layer], count
        )
        msgs = exchange(msg, "sp")
        copies = close_call(position, msgs, cum, state, gate_rows, chips)
        mine = exchange(copies, "x")
        mix = gather(mix_proj[layer], "sp")
        theirs = swap(mine)
        mixed = residual.astype(jnp.float32)
        for piece, weight in zip((mine, theirs), by_core(mix, 0)):
            mixed += jnp.einsum("jct,jcf->tf", piece, weight, preferred_element_type=jnp.float32)
        residual = mixed.astype(jnp.bfloat16)
    return residual


def solution(mesh):
    grid = mesh.devices
    split = Mesh(grid.reshape(*grid.shape[:2], grid.shape[2] // 2, 2), ("grp", "sp", "x", "core"))
    tp = ("x", "core")
    in_specs = (
        P(("grp", "sp"), tp),
        P(),
        P(None, tp, "sp"),
        P(None, tp, "sp"),
        P(None, None, tp),
        P(None, tp, None, None),
        P(None, tp, None, None),
        P(None, tp),
        P(None, tp, "sp"),
        P(None, "sp", tp),
    )
    return jax.shard_map(
        local, mesh=split, in_specs=in_specs, out_specs=P(("grp", "sp"), tp), check_vma=False
    )
```

```python
import jax
import jax.numpy as jnp
from jax import lax
from jax.experimental import pallas as pl
from jax.experimental.pallas import tpu as pltpu
from jax.sharding import Mesh, PartitionSpec as P


LAYERS = 2
EPS = 1e-06
RATE_SCALE = 8.0
LANES = 128


def one_minus_exp(u):
    series = 1.0
    for n in range(9, 1, -1):
        series = 1.0 + u * series * (1.0 / n)
    return jnp.where(u > -0.5, -u * series, 1.0 - jnp.exp(u))


def scan_kernel(value_ref, before_ref, consts_ref, maps_ref, offset_ref, cum_ref, state_ref, msg_ref):
    channels, tok = value_ref.shape
    taps = 4
    value = value_ref[...].astype(jnp.float32)
    full = jnp.concatenate([before_ref[...].astype(jnp.float32), value], axis=1)
    smoothed = consts_ref[:, taps - 1 : taps] * value
    for back in range(1, taps):
        shifted = pltpu.roll(full, back, axis=1)[:, LANES:]
        smoothed = smoothed + consts_ref[:, taps - 1 - back : taps - back] * shifted
    half = smoothed.astype(jnp.bfloat16)
    gates = lax.dot_general(
        maps_ref[...], half, (((1,), (0,)), ((), ())), preferred_element_type=jnp.float32
    )
    gates = 1.0 / (1.0 + jnp.exp(-gates))
    recur, inputs = gates[:channels], gates[channels:]
    log_decay = consts_ref[:, taps : taps + 1] * recur + offset_ref[...]
    a = jnp.exp(log_decay)
    b = jnp.sqrt(one_minus_exp(2.0 * log_decay)) * inputs * smoothed
    lane = lax.broadcasted_iota(jnp.int32, (channels, tok), 1)
    step = 1
    while step < tok:
        inside = lane >= step
        b = jnp.where(inside, a * pltpu.roll(b, step, axis=1), 0.0) + b
        a = jnp.where(inside, pltpu.roll(a, step, axis=1), 1.0) * a
        step *= 2
    cum_ref[...] = a
    state_ref[...] = b
    last = jnp.concatenate([a[:, tok - LANES :], b[:, tok - LANES :]], axis=0)
    row = last.T[LANES - 1 : LANES, :]
    msg_ref[...] = jnp.broadcast_to(row[None], msg_ref.shape)


def close_kernel(pos_ref, msgs_ref, cum_ref, state_ref, gate_ref, out_ref):
    channels, tok = cum_ref.shape
    count = msgs_ref.shape[0]
    position = pos_ref[0]
    carry = jnp.zeros((1, channels), jnp.float32)
    for s in range(count - 1):
        line = msgs_ref[s]
        step = line[:, :channels] * carry + line[:, channels:]
        carry = jnp.where(s < position, step, carry)
    wide = jnp.broadcast_to(carry, (LANES, channels)).T
    wide = jnp.concatenate([wide] * (tok // LANES), axis=1)
    hidden = state_ref[...] + cum_ref[...] * wide
    gate = gate_ref[...].astype(jnp.float32)
    branch = (hidden * (gate / (1.0 + jnp.exp(-gate)))).astype(jnp.bfloat16)
    out_ref[...] = jnp.broadcast_to(branch[None], out_ref.shape)


def project_kernel(ids_ref, mine_ref, theirs_ref, gain_ref, weight_ref, value_ref, gate_ref):
    chips, tok, width = mine_ref.shape
    channels = value_ref.shape[0]
    product = jnp.zeros((2 * channels, tok), jnp.float32)
    squares = jnp.zeros((tok, width), jnp.float32)
    for side, piece_ref in enumerate((mine_ref, theirs_ref)):
        for chip in range(chips):
            at = side * chips + chip
            wide = piece_ref[chip].astype(jnp.float32)
            squares += wide * wide
            scaled = (wide * gain_ref[ids_ref[0, at]]).astype(jnp.bfloat16)
            weight = weight_ref[ids_ref[1, at], : 2 * channels, :]
            product += lax.dot_general(
                weight, scaled, (((1,), (1,)), ((), ())), preferred_element_type=jnp.float32
            )
    mean = jnp.sum(squares.T, axis=0, keepdims=True) * (1.0 / (2 * chips * width))
    rows = (product * lax.rsqrt(mean + EPS)).astype(jnp.bfloat16)
    value_ref[...] = rows[:channels]
    gate_ref[...] = rows[channels:]


def mix_kernel(ids_ref, mine_ref, theirs_ref, weight_ref, residual_ref, out_ref):
    chips, channels, _ = mine_ref.shape
    first = weight_ref.shape[1] - channels
    mixed = residual_ref[...].astype(jnp.float32)
    for chip in range(chips):
        branch = jnp.concatenate([mine_ref[chip], theirs_ref[chip]], axis=0)
        weight = jnp.concatenate(
            [weight_ref[ids_ref[1, side * chips + chip], first:, :] for side in range(2)], axis=0
        )
        mixed += lax.dot_general(
            branch, weight, (((0,), (0,)), ((), ())), preferred_element_type=jnp.float32
        )
    mixed = mixed.astype(jnp.bfloat16)
    if len(out_ref.shape) == 3:
        mixed = jnp.broadcast_to(mixed[None], out_ref.shape)
    out_ref[...] = mixed


def vmem(n):
    return [pl.BlockSpec(memory_space=pltpu.VMEM)] * n


def smem(n):
    return [pl.BlockSpec(memory_space=pltpu.SMEM)] * n


def project_call(ids, mine, theirs, gains, weights):
    _, tok, _ = mine.shape
    channels = weights.shape[1] // 3
    rows = jax.ShapeDtypeStruct((channels, tok), jnp.bfloat16)
    return pl.pallas_call(
        project_kernel,
        out_shape=(rows, rows),
        in_specs=smem(1) + vmem(4),
        out_specs=tuple(vmem(2)),
        name="project",
    )(ids, mine, theirs, gains, weights)


def mix_call(ids, mine, theirs, weights, residual, copies):
    return pl.pallas_call(
        mix_kernel,
        out_shape=jax.ShapeDtypeStruct(copies + residual.shape, jnp.bfloat16),
        in_specs=smem(1) + vmem(4),
        out_specs=vmem(1)[0],
        name="mix",
    )(ids, mine, theirs, weights, residual)


def scan_call(value, before, consts, maps, offset, count):
    channels, tok = value.shape
    return pl.pallas_call(
        scan_kernel,
        out_shape=(
            jax.ShapeDtypeStruct((channels, tok), jnp.float32),
            jax.ShapeDtypeStruct((channels, tok), jnp.float32),
            jax.ShapeDtypeStruct((count, 1, 2 * channels), jnp.float32),
        ),
        in_specs=vmem(5),
        out_specs=tuple(vmem(3)),
        name="scan",
    )(value, before, consts, maps, offset)


def close_call(position, msgs, cum, state, gate, copies):
    channels, tok = cum.shape
    return pl.pallas_call(
        close_kernel,
        out_shape=jax.ShapeDtypeStruct((copies, channels, tok), jnp.bfloat16),
        in_specs=smem(1) + vmem(4),
        out_specs=vmem(1)[0],
        name="close",
    )(position, msgs, cum, state, gate)


def exchange(copies, axis):
    return lax.all_to_all(copies, axis, split_axis=0, concat_axis=0, tiled=True)


def shift(array, axis, steps):
    count = lax.axis_size(axis)
    return lax.ppermute(array, axis, [(i, (i + steps) % count) for i in range(count)])


NEAR = (-2, -1, 0, 1)


def far_hops(array, axis):
    far = lax.axis_size(axis) // len(NEAR)
    return jnp.stack([array] + [shift(array, axis, len(NEAR) * q) for q in range(1, far)])


def near_hops(held, axis):
    return jnp.concatenate([shift(held, axis, n) if n else held for n in NEAR])


def slot_of(behind, count):
    at = (behind - NEAR[0]) % count
    return at % len(NEAR) * (count // len(NEAR)) + at // len(NEAR)


def local(
    tokens,
    norm_gain,
    value_proj,
    gate_proj,
    conv_taps,
    recur_map,
    input_map,
    decay_param,
    decay_offset,
    mix_proj,
):
    tok_rows, own_cols = tokens.shape
    chips, cores, count = lax.axis_size("x"), lax.axis_size("core"), lax.axis_size("sp")
    chip, core, place = lax.axis_index("x"), lax.axis_index("core"), lax.axis_index("sp")

    def swap(array):
        return shift(array, "core", 1)

    rates = -RATE_SCALE * jax.nn.softplus(-decay_param)
    consts = jnp.concatenate([conv_taps.transpose(0, 2, 1), rates[:, :, None]], axis=2)
    consts = jnp.pad(consts, ((0, 0), (0, 0), (0, LANES - consts.shape[2])))
    maps = jnp.concatenate([recur_map[:, 0], input_map[:, 0]], axis=2).transpose(0, 2, 1)
    gains = norm_gain.reshape(LAYERS, chips * cores, 1, own_cols)
    shards = jnp.concatenate([value_proj, gate_proj, mix_proj], axis=1)

    slots = jnp.arange(chips)
    far = chips // len(NEAR)
    behind = slots % far * len(NEAR) + slots // far + NEAR[0]
    sides = jnp.stack([core, 1 - core])[:, None]
    by_slot = (cores * ((chip - behind) % chips)[None, :] + sides).reshape(-1)
    by_chip = (cores * slots[None, :] + sides).reshape(-1)
    by_hops = slot_of(place - by_chip, count)
    first_ids = jnp.stack([by_slot, by_slot]).astype(jnp.int32)
    plain_ids = jnp.stack([by_chip, by_chip]).astype(jnp.int32)
    hop_ids = jnp.stack([by_chip, by_hops]).astype(jnp.int32)

    first_weights = exchange(jnp.broadcast_to(shards[0], (count, *shards[0].shape)), "sp")
    first_tokens = near_hops(far_hops(tokens, "x"), "x")
    residual = tokens
    for layer in range(LAYERS):
        if layer == 0:
            mine, weights, ids, mix_ids = first_tokens, first_weights, first_ids, plain_ids
        else:
            mine, ids, mix_ids = None, hop_ids, hop_ids
        if mine is None:
            _, held = lax.optimization_barrier((copies, held))
            mine = exchange(copies, "x")
            weights = near_hops(held, "sp")
        theirs = swap(mine)
        value_rows, gate_rows = project_call(ids, mine, theirs, gains[layer], weights)
        before = lax.ppermute(
            value_rows[:, tok_rows - LANES :], "sp", [(i, i + 1) for i in range(count - 1)]
        )
        cum, state, msg = scan_call(
            value_rows, before, consts[layer], maps[layer], decay_offset[layer], count
        )
        msgs = exchange(msg, "sp")
        sent = close_call(place.reshape(1), msgs, cum, state, gate_rows, chips)
        if layer + 1 < LAYERS:
            _, shard = lax.optimization_barrier((sent, shards[layer + 1]))
        mine = exchange(sent, "x")
        if layer + 1 < LAYERS:
            held = far_hops(shard, "sp")
        theirs = swap(mine)
        if layer + 1 < LAYERS:
            copies = mix_call(mix_ids, mine, theirs, weights, residual, (chips,))
            residual = copies[0]
        else:
            residual = mix_call(mix_ids, mine, theirs, weights, residual, ())
    return residual


def solution(mesh):
    grid = mesh.devices
    split = Mesh(grid.reshape(*grid.shape[:2], grid.shape[2] // 2, 2), ("grp", "sp", "x", "core"))
    tp = ("x", "core")
    in_specs = (
        P(("grp", "sp"), tp),
        P(),
        P(None, tp, "sp"),
        P(None, tp, "sp"),
        P(None, None, tp),
        P(None, tp, None, None),
        P(None, tp, None, None),
        P(None, tp),
        P(None, tp, "sp"),
        P(None, "sp", tp),
    )
    return jax.shard_map(
        local, mesh=split, in_specs=in_specs, out_specs=P(("grp", "sp"), tp), check_vma=False
    )
```

```python
import functools

import jax
import jax.numpy as jnp
from jax import lax
from jax.experimental import pallas as pl
from jax.experimental.pallas import tpu as pltpu
from jax.sharding import Mesh, PartitionSpec as P


LAYERS = 2
EPS = 1e-06
RATE_SCALE = 8.0
LANES = 128


def one_minus_exp(u):
    series = 1.0
    for n in range(9, 1, -1):
        series = 1.0 + u * series * (1.0 / n)
    return jnp.where(u > -0.5, -u * series, 1.0 - jnp.exp(u))


def scan_kernel(
    layer, value_ref, before_ref, consts_ref, maps_ref, offset_ref, cum_ref, state_ref, msg_ref
):
    channels, tok = value_ref.shape
    taps = 4
    value = value_ref[...].astype(jnp.float32)
    full = jnp.concatenate([before_ref[...].astype(jnp.float32), value], axis=1)
    consts = consts_ref[layer]
    smoothed = consts[:, taps - 1 : taps] * value
    for back in range(1, taps):
        shifted = pltpu.roll(full, back, axis=1)[:, LANES:]
        smoothed = smoothed + consts[:, taps - 1 - back : taps - back] * shifted
    half = smoothed.astype(jnp.bfloat16)
    gates = lax.dot_general(
        maps_ref[layer], half, (((1,), (0,)), ((), ())), preferred_element_type=jnp.float32
    )
    gates = 1.0 / (1.0 + jnp.exp(-gates))
    recur, inputs = gates[:channels], gates[channels:]
    log_decay = consts[:, taps : taps + 1] * recur + offset_ref[layer]
    a = jnp.exp(log_decay)
    b = jnp.sqrt(one_minus_exp(2.0 * log_decay)) * inputs * smoothed
    lane = lax.broadcasted_iota(jnp.int32, (channels, tok), 1)
    step = 1
    while step < tok:
        inside = lane >= step
        b = jnp.where(inside, a * pltpu.roll(b, step, axis=1), 0.0) + b
        a = jnp.where(inside, pltpu.roll(a, step, axis=1), 1.0) * a
        step *= 2
    cum_ref[...] = a
    state_ref[...] = b
    last = jnp.concatenate([a[:, tok - LANES :], b[:, tok - LANES :]], axis=0)
    row = last.T[LANES - 1 : LANES, :]
    msg_ref[...] = jnp.broadcast_to(row[None], msg_ref.shape)


def close_kernel(pos_ref, msgs_ref, cum_ref, state_ref, gate_ref, out_ref):
    channels, tok = cum_ref.shape
    count = msgs_ref.shape[0]
    position = pos_ref[0]
    carry = jnp.zeros((1, channels), jnp.float32)
    for s in range(count - 1):
        line = msgs_ref[s]
        step = line[:, :channels] * carry + line[:, channels:]
        carry = jnp.where(s < position, step, carry)
    wide = jnp.broadcast_to(carry, (LANES, channels)).T
    wide = jnp.concatenate([wide] * (tok // LANES), axis=1)
    hidden = state_ref[...] + cum_ref[...] * wide
    gate = gate_ref[...].astype(jnp.float32)
    branch = (hidden * (gate / (1.0 + jnp.exp(-gate)))).astype(jnp.bfloat16)
    out_ref[...] = jnp.broadcast_to(branch[None], out_ref.shape)


def project_kernel(
    layer, ids_ref, mine_ref, theirs_ref, gain_ref, weight_ref, value_ref, gate_ref, tail_ref
):
    chips, tok, width = mine_ref.shape
    channels = value_ref.shape[0]
    product = jnp.zeros((2 * channels, tok), jnp.float32)
    squares = jnp.zeros((tok, width), jnp.float32)
    for side, piece_ref in enumerate((mine_ref, theirs_ref)):
        for chip in range(chips):
            at = side * chips + chip
            wide = piece_ref[chip].astype(jnp.float32)
            squares += wide * wide
            scaled = (wide * gain_ref[layer, ids_ref[0, at]]).astype(jnp.bfloat16)
            weight = weight_ref[ids_ref[1, at], : 2 * channels, :]
            product += lax.dot_general(
                weight, scaled, (((1,), (1,)), ((), ())), preferred_element_type=jnp.float32
            )
    mean = jnp.sum(squares.T, axis=0, keepdims=True) * (1.0 / (2 * chips * width))
    rows = (product * lax.rsqrt(mean + EPS)).astype(jnp.bfloat16)
    value_ref[...] = rows[:channels]
    gate_ref[...] = rows[channels:]
    tail_ref[...] = rows[:channels, tok - LANES :]


def mix_kernel(ids_ref, mine_ref, theirs_ref, weight_ref, residual_ref, out_ref, *copies_ref):
    chips, channels, _ = mine_ref.shape
    first = weight_ref.shape[1] - channels
    mixed = residual_ref[...].astype(jnp.float32)
    for chip in range(chips):
        branch = jnp.concatenate([mine_ref[chip], theirs_ref[chip]], axis=0)
        weight = jnp.concatenate(
            [weight_ref[ids_ref[1, side * chips + chip], first:, :] for side in range(2)], axis=0
        )
        mixed += lax.dot_general(
            branch, weight, (((0,), (0,)), ((), ())), preferred_element_type=jnp.float32
        )
    mixed = mixed.astype(jnp.bfloat16)
    out_ref[...] = mixed
    for ref in copies_ref:
        ref[...] = jnp.broadcast_to(mixed[None], ref.shape)


def vmem(n):
    return [pl.BlockSpec(memory_space=pltpu.VMEM)] * n


def smem(n):
    return [pl.BlockSpec(memory_space=pltpu.SMEM)] * n


def project_call(layer, ids, mine, theirs, gains, weights):
    _, tok, _ = mine.shape
    channels = weights.shape[1] // 3
    rows = jax.ShapeDtypeStruct((channels, tok), jnp.bfloat16)
    return pl.pallas_call(
        functools.partial(project_kernel, layer),
        out_shape=(rows, rows, jax.ShapeDtypeStruct((channels, LANES), jnp.bfloat16)),
        in_specs=smem(1) + vmem(4),
        out_specs=tuple(vmem(3)),
        name="project",
    )(ids, mine, theirs, gains, weights)


def mix_call(ids, mine, theirs, weights, residual, copies):
    shapes = [residual.shape] + ([(copies, *residual.shape)] if copies else [])
    return pl.pallas_call(
        mix_kernel,
        out_shape=[jax.ShapeDtypeStruct(shape, jnp.bfloat16) for shape in shapes],
        in_specs=smem(1) + vmem(4),
        out_specs=vmem(len(shapes)),
        name="mix",
    )(ids, mine, theirs, weights, residual)


def scan_call(layer, value, before, consts, maps, offset, count):
    channels, tok = value.shape
    return pl.pallas_call(
        functools.partial(scan_kernel, layer),
        out_shape=(
            jax.ShapeDtypeStruct((channels, tok), jnp.float32),
            jax.ShapeDtypeStruct((channels, tok), jnp.float32),
            jax.ShapeDtypeStruct((count, 1, 2 * channels), jnp.float32),
        ),
        in_specs=vmem(5),
        out_specs=tuple(vmem(3)),
        name="scan",
    )(value, before, consts, maps, offset)


def close_call(position, msgs, cum, state, gate, copies):
    channels, tok = cum.shape
    return pl.pallas_call(
        close_kernel,
        out_shape=jax.ShapeDtypeStruct((copies, channels, tok), jnp.bfloat16),
        in_specs=smem(1) + vmem(4),
        out_specs=vmem(1)[0],
        name="close",
    )(position, msgs, cum, state, gate)


def tick_kernel(ids_ref, out_ref):
    for side in range(ids_ref.shape[0]):
        for at in range(ids_ref.shape[1]):
            out_ref[side, at] = ids_ref[side, at]


def tick_call(ids):
    return pl.pallas_call(
        tick_kernel,
        out_shape=jax.ShapeDtypeStruct(ids.shape, ids.dtype),
        in_specs=smem(1),
        out_specs=smem(1)[0],
        name="copy_ids",
    )(ids)


def exchange(copies, axis):
    return lax.all_to_all(copies, axis, split_axis=0, concat_axis=0, tiled=True)


def shift(array, axis, steps):
    count = lax.axis_size(axis)
    return lax.ppermute(array, axis, [(i, (i + steps) % count) for i in range(count)])


NEAR = (-2, -1, 0, 1)


def far_hops(array, axis):
    far = lax.axis_size(axis) // len(NEAR)
    return jnp.stack([array] + [shift(array, axis, len(NEAR) * q) for q in range(1, far)])


def near_hops(held, axis):
    return jnp.concatenate([shift(held, axis, n) if n else held for n in NEAR])


def slot_of(behind, count):
    at = (behind - NEAR[0]) % count
    return at % len(NEAR) * (count // len(NEAR)) + at // len(NEAR)


def local(
    tokens,
    norm_gain,
    value_proj,
    gate_proj,
    conv_taps,
    recur_map,
    input_map,
    decay_param,
    decay_offset,
    mix_proj,
):
    _, own_cols = tokens.shape
    chips, cores, count = lax.axis_size("x"), lax.axis_size("core"), lax.axis_size("sp")
    chip, core, place = lax.axis_index("x"), lax.axis_index("core"), lax.axis_index("sp")

    def swap(array):
        return shift(array, "core", 1)

    rates = -RATE_SCALE * jax.nn.softplus(-decay_param)
    consts = jnp.concatenate([conv_taps.transpose(0, 2, 1), rates[:, :, None]], axis=2)
    consts = jnp.pad(consts, ((0, 0), (0, 0), (0, LANES - consts.shape[2])))
    maps = jnp.concatenate([recur_map[:, 0], input_map[:, 0]], axis=2).transpose(0, 2, 1)
    gains = norm_gain.reshape(LAYERS, chips * cores, 1, own_cols)
    shards = jnp.concatenate([value_proj, gate_proj, mix_proj], axis=1)

    slots = jnp.arange(chips)
    far = chips // len(NEAR)
    behind = slots % far * len(NEAR) + slots // far + NEAR[0]
    sides = jnp.stack([core, 1 - core])[:, None]
    by_slot = (cores * ((chip - behind) % chips)[None, :] + sides).reshape(-1)
    by_chip = (cores * slots[None, :] + sides).reshape(-1)
    by_hops = slot_of(place - by_chip, count)
    first_ids = jnp.stack([by_slot, by_slot]).astype(jnp.int32)
    plain_ids = jnp.stack([by_chip, by_chip]).astype(jnp.int32)
    hop_ids = tick_call(jnp.stack([by_chip, by_hops]).astype(jnp.int32))
    hop_ids = tick_call(hop_ids)

    first_weights = exchange(jnp.broadcast_to(shards[0], (count, *shards[0].shape)), "sp")
    first_tokens = near_hops(far_hops(tokens, "x"), "x")
    residual = tokens
    for layer in range(LAYERS):
        if layer == 0:
            mine, weights, ids, mix_ids = first_tokens, first_weights, first_ids, plain_ids
        else:
            mine, weights, ids, mix_ids = None, later_weights, hop_ids, hop_ids
        if mine is None:
            mine = exchange(copies[0], "x")
        theirs = swap(mine)
        value_rows, gate_rows, tail = project_call(
            layer, ids, mine, theirs, gains, weights
        )
        before = lax.ppermute(tail, "sp", [(i, i + 1) for i in range(count - 1)])
        cum, state, msg = scan_call(layer, value_rows, before, consts, maps, decay_offset, count)
        msgs = exchange(msg, "sp")
        if layer + 1 < LAYERS:
            _, shard = lax.optimization_barrier((msg, shards[layer + 1]))
            held = far_hops(shard, "sp")
        sent = close_call(place.reshape(1), msgs, cum, state, gate_rows, chips)
        mine = exchange(sent, "x")
        if layer + 1 < LAYERS:
            _, held = lax.optimization_barrier((sent, held))
            later_weights = near_hops(held, "sp")
        theirs = swap(mine)
        residual, *copies = mix_call(
            mix_ids, mine, theirs, weights, residual, chips if layer + 1 < LAYERS else 0
        )
    return residual


def solution(mesh):
    grid = mesh.devices
    split = Mesh(grid.reshape(*grid.shape[:2], grid.shape[2] // 2, 2), ("grp", "sp", "x", "core"))
    tp = ("x", "core")
    in_specs = (
        P(("grp", "sp"), tp),
        P(),
        P(None, tp, "sp"),
        P(None, tp, "sp"),
        P(None, None, tp),
        P(None, tp, None, None),
        P(None, tp, None, None),
        P(None, tp),
        P(None, tp, "sp"),
        P(None, "sp", tp),
    )
    return jax.shard_map(
        local, mesh=split, in_specs=in_specs, out_specs=P(("grp", "sp"), tp), check_vma=False
    )
```

```python
import functools

import jax
import jax.numpy as jnp
from jax import lax
from jax.experimental import pallas as pl
from jax.experimental.pallas import tpu as pltpu
from jax.sharding import Mesh, PartitionSpec as P


LAYERS = 2
EPS = 1e-06
RATE_SCALE = 8.0
LANES = 128
NEAR = (-2, -1, 0, 1)


def one_minus_exp(u):
    series = 1.0
    for n in range(9, 1, -1):
        series = 1.0 + u * series * (1.0 / n)
    return jnp.where(u > -0.5, -u * series, 1.0 - jnp.exp(u))


def scan_kernel(
    layer, value_ref, before_ref, consts_ref, maps_ref, offset_ref, cum_ref, state_ref, msg_ref
):
    channels, tok = value_ref.shape
    taps = 4
    value = value_ref[...].astype(jnp.float32)
    full = jnp.concatenate([before_ref[...].astype(jnp.float32), value], axis=1)
    consts = consts_ref[layer]
    smoothed = consts[:, taps - 1 : taps] * value
    for back in range(1, taps):
        shifted = pltpu.roll(full, back, axis=1)[:, LANES:]
        smoothed = smoothed + consts[:, taps - 1 - back : taps - back] * shifted
    half = smoothed.astype(jnp.bfloat16)
    gates = lax.dot_general(
        maps_ref[layer], half, (((1,), (0,)), ((), ())), preferred_element_type=jnp.float32
    )
    gates = 1.0 / (1.0 + jnp.exp(-gates))
    recur, inputs = gates[:channels], gates[channels:]
    log_decay = consts[:, taps : taps + 1] * recur + offset_ref[layer]
    a = jnp.exp(log_decay)
    b = jnp.sqrt(one_minus_exp(2.0 * log_decay)) * inputs * smoothed
    lane = lax.broadcasted_iota(jnp.int32, (channels, tok), 1)
    step = 1
    while step < tok:
        inside = lane >= step
        b = jnp.where(inside, a * pltpu.roll(b, step, axis=1), 0.0) + b
        a = jnp.where(inside, pltpu.roll(a, step, axis=1), 1.0) * a
        step *= 2
    cum_ref[...] = a
    state_ref[...] = b
    last = jnp.concatenate([a[:, tok - LANES :], b[:, tok - LANES :]], axis=0)
    row = last.T[LANES - 1 : LANES, :]
    msg_ref[...] = jnp.broadcast_to(row[None], msg_ref.shape)


def close_kernel(msgs_ref, cum_ref, state_ref, gate_ref, out_ref):
    channels, tok = cum_ref.shape
    count = msgs_ref.shape[0]
    position = lax.axis_index("sp")
    carry = jnp.zeros((1, channels), jnp.float32)
    for s in range(count - 1):
        line = msgs_ref[s]
        step = line[:, :channels] * carry + line[:, channels:]
        carry = jnp.where(s < position, step, carry)
    wide = jnp.broadcast_to(carry, (LANES, channels)).T
    wide = jnp.concatenate([wide] * (tok // LANES), axis=1)
    hidden = state_ref[...] + cum_ref[...] * wide
    gate = gate_ref[...].astype(jnp.float32)
    branch = (hidden * (gate / (1.0 + jnp.exp(-gate)))).astype(jnp.bfloat16)
    out_ref[...] = jnp.broadcast_to(branch[None], out_ref.shape)


def blocks_of(chips, count, hopped, slotted=False):
    chip, core, place = (lax.axis_index(name) for name in ("x", "core", "sp"))
    far = chips // len(NEAR)
    for side in range(2):
        for slot in range(chips):
            source = slot
            if slotted:
                behind = slot % far * len(NEAR) + slot // far + NEAR[0]
                source = lax.rem(chip + chips - behind, chips)
            block = 2 * source + (core if side == 0 else 1 - core)
            held = block
            if hopped:
                at = lax.rem(place + 2 * count - block - NEAR[0], count)
                held = lax.rem(at, len(NEAR)) * (count // len(NEAR)) + lax.div(at, len(NEAR))
            yield side, slot, block, held


def project_kernel(
    slotted, hopped, mine_ref, theirs_ref, gain_ref, weight_ref, value_ref, gate_ref, tail_ref
):
    chips, tok, width = mine_ref.shape
    channels = value_ref.shape[0]
    product = jnp.zeros((2 * channels, tok), jnp.float32)
    squares = jnp.zeros((tok, width), jnp.float32)
    pieces = (mine_ref, theirs_ref)
    for side, slot, block, held in blocks_of(chips, weight_ref.shape[0], hopped, slotted):
        wide = pieces[side][slot].astype(jnp.float32)
        squares += wide * wide
        scaled = (wide * gain_ref[block]).astype(jnp.bfloat16)
        product += lax.dot_general(
            weight_ref[held, : 2 * channels, :],
            scaled,
            (((1,), (1,)), ((), ())),
            preferred_element_type=jnp.float32,
        )
    mean = jnp.sum(squares.T, axis=0, keepdims=True) * (1.0 / (2 * chips * width))
    rows = (product * lax.rsqrt(mean + EPS)).astype(jnp.bfloat16)
    value_ref[...] = rows[:channels]
    gate_ref[...] = rows[channels:]
    tail_ref[...] = rows[:channels, tok - LANES :]


def mix_kernel(hopped, mine_ref, theirs_ref, weight_ref, residual_ref, out_ref, *copies_ref):
    chips, channels, _ = mine_ref.shape
    first = weight_ref.shape[1] - channels
    held = {(side, slot): w for side, slot, _, w in blocks_of(chips, weight_ref.shape[0], hopped)}
    mixed = residual_ref[...].astype(jnp.float32)
    for slot in range(chips):
        branch = jnp.concatenate([mine_ref[slot], theirs_ref[slot]], axis=0)
        weight = jnp.concatenate(
            [weight_ref[held[side, slot], first:, :] for side in range(2)], axis=0
        )
        mixed += lax.dot_general(
            branch, weight, (((0,), (0,)), ((), ())), preferred_element_type=jnp.float32
        )
    mixed = mixed.astype(jnp.bfloat16)
    out_ref[...] = mixed
    for ref in copies_ref:
        ref[...] = jnp.broadcast_to(mixed[None], ref.shape)


def pack_kernel(value_ref, gate_ref, mix_ref, *out_refs):
    for layer, out_ref in enumerate(out_refs):
        rows = jnp.concatenate([value_ref[layer], gate_ref[layer], mix_ref[layer]], axis=0)
        if len(out_ref.shape) == 3:
            rows = jnp.broadcast_to(rows[None], out_ref.shape)
        out_ref[...] = rows


def vmem(n):
    return [pl.BlockSpec(memory_space=pltpu.VMEM)] * n


def kernel_call(kernel, out_shape, *operands):
    return pl.pallas_call(
        kernel, out_shape=out_shape, in_specs=vmem(len(operands)), out_specs=vmem(len(out_shape))
    )(*(pltpu.with_memory_space_constraint(a, pltpu.VMEM) for a in operands))


def pack_call(value_proj, gate_proj, mix_proj, count):
    layers, channels, width = value_proj.shape
    rows = (3 * channels, width)
    out = [pltpu.VMEM((count, *rows), value_proj.dtype)]
    out += [pltpu.VMEM(rows, value_proj.dtype)] * (layers - 1)
    return kernel_call(pack_kernel, out, value_proj, gate_proj, mix_proj)


def project_call(slotted, hopped, mine, theirs, gains, weights):
    _, tok, _ = mine.shape
    channels = weights.shape[1] // 3
    out = [pltpu.VMEM((channels, n), jnp.bfloat16) for n in (tok, tok, LANES)]
    kernel = functools.partial(project_kernel, slotted, hopped)
    return kernel_call(kernel, out, mine, theirs, gains, weights)


def mix_call(hopped, mine, theirs, weights, residual, copies):
    shape, dtype = residual.shape, jnp.bfloat16
    if copies:
        out = [pltpu.VMEM(shape, dtype), pltpu.VMEM((copies, *shape), dtype)]
    else:
        out = [jax.ShapeDtypeStruct(shape, dtype)]
    kernel = functools.partial(mix_kernel, hopped)
    return kernel_call(kernel, out, mine, theirs, weights, residual)


def scan_call(layer, value, before, consts, maps, offset, count):
    channels, tok = value.shape
    out = [
        pltpu.VMEM((channels, tok), jnp.float32),
        pltpu.VMEM((channels, tok), jnp.float32),
        pltpu.VMEM((count, 1, 2 * channels), jnp.float32),
    ]
    kernel = functools.partial(scan_kernel, layer)
    return kernel_call(kernel, out, value, before, consts, maps, offset)


def close_call(msgs, cum, state, gate, copies):
    out = [pltpu.VMEM((copies, *cum.shape), jnp.bfloat16)]
    return kernel_call(close_kernel, out, msgs, cum, state, gate)[0]


def copy_kernel(in_ref, out_ref):
    out_ref[...] = in_ref[...]


def copy_call(array):
    return kernel_call(copy_kernel, [pltpu.VMEM(array.shape, array.dtype)], array)[0]


def exchange(copies, axis):
    return lax.all_to_all(copies, axis, split_axis=0, concat_axis=0, tiled=True)


def shift(array, axis, steps):
    count = lax.axis_size(axis)
    return lax.ppermute(array, axis, [(i, (i + steps) % count) for i in range(count)])


def far_hop(array, axis, hops=1):
    return shift(array, axis, len(NEAR) * hops)


def near_hops(held, axis):
    return jnp.concatenate([shift(held, axis, n) if n else held for n in NEAR])


def local(
    tokens,
    norm_gain,
    value_proj,
    gate_proj,
    conv_taps,
    recur_map,
    input_map,
    decay_param,
    decay_offset,
    mix_proj,
):
    own_cols = tokens.shape[1]
    chips, cores, count = (lax.axis_size(name) for name in ("x", "core", "sp"))

    def swap(array):
        return shift(array, "core", 1)

    first, shard = pack_call(value_proj, gate_proj, mix_proj, count)
    weights = exchange(first, "sp")
    held = jnp.stack([tokens, far_hop(tokens, "x")])
    mine = near_hops(held, "x")
    rates = -RATE_SCALE * jax.nn.softplus(-decay_param)
    consts = jnp.concatenate([conv_taps.transpose(0, 2, 1), rates[:, :, None]], axis=2)
    consts = jnp.pad(consts, ((0, 0), (0, 0), (0, LANES - consts.shape[2])))
    maps = jnp.concatenate([recur_map[:, 0], input_map[:, 0]], axis=2).transpose(0, 2, 1)
    gains = [gain.reshape(chips * cores, 1, own_cols) for gain in norm_gain]
    gains[1] = copy_call(gains[1])
    gains[1] = copy_call(gains[1])

    residual = tokens
    for layer in range(LAYERS):
        more = layer + 1 < LAYERS
        if layer:
            mine = exchange(copies[0], "x")
            weights = later_weights
        theirs = swap(mine)
        value_rows, gate_rows, tail = project_call(
            layer == 0, layer > 0, mine, theirs, gains[layer], weights
        )
        before = lax.ppermute(tail, "sp", [(i, i + 1) for i in range(count - 1)])
        cum, state, msg = scan_call(layer, value_rows, before, consts, maps, decay_offset, count)
        msgs = exchange(msg, "sp")
        if more:
            _, shard = lax.optimization_barrier((msg, shard))
            hop_one = far_hop(shard, "sp")
        sent = close_call(msgs, cum, state, gate_rows, chips)
        mine = exchange(sent, "x")
        if more:
            _, shard, hop_one = lax.optimization_barrier((sent, shard, hop_one))
            hop_back = far_hop(shard, "sp", -1)
            hop_two = far_hop(hop_one, "sp")
        theirs = swap(mine)
        residual, *copies = mix_call(
            layer > 0, mine, theirs, weights, residual, chips if more else 0
        )
        if more:
            _, *held = lax.optimization_barrier((copies[0], shard, hop_one, hop_two, hop_back))
            later_weights = near_hops(jnp.stack(held), "sp")
    return residual


def solution(mesh):
    grid = mesh.devices
    split = Mesh(grid.reshape(*grid.shape[:2], grid.shape[2] // 2, 2), ("grp", "sp", "x", "core"))
    tp = ("x", "core")
    in_specs = (
        P(("grp", "sp"), tp),
        P(),
        P(None, tp, "sp"),
        P(None, tp, "sp"),
        P(None, None, tp),
        P(None, tp, None, None),
        P(None, tp, None, None),
        P(None, tp),
        P(None, tp, "sp"),
        P(None, "sp", tp),
    )
    return jax.shard_map(
        local, mesh=split, in_specs=in_specs, out_specs=P(("grp", "sp"), tp), check_vma=False
    )
```

```python
import functools

import jax
import jax.numpy as jnp
from jax import lax
from jax.experimental import pallas as pl
from jax.experimental.pallas import tpu as pltpu
from jax.sharding import Mesh, PartitionSpec as P


LAYERS = 2
EPS = 1e-06
RATE_SCALE = 8.0
LANES = 128
NEAR = (-2, -1, 0, 1)


def one_minus_exp(u):
    series = 1.0
    for n in range(9, 1, -1):
        series = 1.0 + u * series * (1.0 / n)
    return jnp.where(u > -0.5, -u * series, 1.0 - jnp.exp(u))


def scan_kernel(
    layer, value_ref, before_ref, consts_ref, maps_ref, offset_ref, cum_ref, state_ref, msg_ref
):
    channels, tok = value_ref.shape
    taps = 4
    value = value_ref[...].astype(jnp.float32)
    full = jnp.concatenate([before_ref[...].astype(jnp.float32), value], axis=1)
    consts = consts_ref[layer]
    smoothed = consts[:, taps - 1 : taps] * value
    for back in range(1, taps):
        shifted = pltpu.roll(full, back, axis=1)[:, LANES:]
        smoothed = smoothed + consts[:, taps - 1 - back : taps - back] * shifted
    half = smoothed.astype(jnp.bfloat16)
    gates = lax.dot_general(
        maps_ref[layer], half, (((1,), (0,)), ((), ())), preferred_element_type=jnp.float32
    )
    gates = 1.0 / (1.0 + jnp.exp(-gates))
    recur, inputs = gates[:channels], gates[channels:]
    log_decay = consts[:, taps : taps + 1] * recur + offset_ref[layer]
    a = jnp.exp(log_decay)
    b = jnp.sqrt(one_minus_exp(2.0 * log_decay)) * inputs * smoothed
    lane = lax.broadcasted_iota(jnp.int32, (channels, tok), 1)
    step = 1
    while step < tok:
        inside = lane >= step
        b = jnp.where(inside, a * pltpu.roll(b, step, axis=1), 0.0) + b
        a = jnp.where(inside, pltpu.roll(a, step, axis=1), 1.0) * a
        step *= 2
    cum_ref[...] = a
    state_ref[...] = b
    last = jnp.concatenate([a[:, tok - LANES :], b[:, tok - LANES :]], axis=0)
    row = last.T[LANES - 1 : LANES, :]
    msg_ref[...] = jnp.broadcast_to(row[None], msg_ref.shape)


def close_kernel(msgs_ref, cum_ref, state_ref, gate_ref, out_ref):
    channels, tok = cum_ref.shape
    count = msgs_ref.shape[0]
    position = lax.axis_index("sp")
    carry = jnp.zeros((1, channels), jnp.float32)
    for s in range(count - 1):
        line = msgs_ref[s]
        step = line[:, :channels] * carry + line[:, channels:]
        carry = jnp.where(s < position, step, carry)
    wide = jnp.broadcast_to(carry, (LANES, channels)).T
    wide = jnp.concatenate([wide] * (tok // LANES), axis=1)
    hidden = state_ref[...] + cum_ref[...] * wide
    gate = gate_ref[...].astype(jnp.float32)
    branch = (hidden * (gate / (1.0 + jnp.exp(-gate)))).astype(jnp.bfloat16)
    out_ref[...] = jnp.broadcast_to(branch[None], out_ref.shape)


def blocks_of(chips, count, hopped, slotted=False):
    chip, core, place = (lax.axis_index(name) for name in ("x", "core", "sp"))
    steps = len(NEAR)
    own_sign = 1 - 2 * core
    for side in range(2):
        for slot in range(chips):
            source, sign = slot, own_sign if side == 0 else -own_sign
            if slotted:
                far = chips // steps
                behind = slot % far * steps + sign * NEAR[slot // far]
                source = lax.rem(chip + 2 * chips - behind, chips)
            block = 2 * source + (core if side == 0 else 1 - core)
            held = block
            if hopped:
                far = count // steps
                at = lax.rem(own_sign * (place - block) + 2 * count - NEAR[0], count)
                held = lax.rem(at, steps) * far + lax.rem(own_sign * lax.div(at, steps) + far, far)
            yield side, slot, block, held


def project_kernel(
    slotted, hopped, mine_ref, theirs_ref, gain_ref, weight_ref, value_ref, gate_ref, tail_ref
):
    chips, tok, width = mine_ref.shape
    channels = value_ref.shape[0]
    product = jnp.zeros((2 * channels, tok), jnp.float32)
    squares = jnp.zeros((tok, width), jnp.float32)
    pieces = (mine_ref, theirs_ref)
    for side, slot, block, held in blocks_of(chips, weight_ref.shape[0], hopped, slotted):
        wide = pieces[side][slot].astype(jnp.float32)
        squares += wide * wide
        scaled = (wide * gain_ref[block]).astype(jnp.bfloat16)
        product += lax.dot_general(
            weight_ref[held, : 2 * channels, :],
            scaled,
            (((1,), (1,)), ((), ())),
            preferred_element_type=jnp.float32,
        )
    mean = jnp.sum(squares.T, axis=0, keepdims=True) * (1.0 / (2 * chips * width))
    rows = (product * lax.rsqrt(mean + EPS)).astype(jnp.bfloat16)
    value_ref[...] = rows[:channels]
    gate_ref[...] = rows[channels:]
    tail_ref[...] = rows[:channels, tok - LANES :]


def mix_kernel(hopped, mine_ref, theirs_ref, weight_ref, residual_ref, out_ref, *copies_ref):
    chips, channels, _ = mine_ref.shape
    first = weight_ref.shape[1] - channels
    held = {(side, slot): w for side, slot, _, w in blocks_of(chips, weight_ref.shape[0], hopped)}
    mixed = residual_ref[...].astype(jnp.float32)
    for slot in range(chips):
        branch = jnp.concatenate([mine_ref[slot], theirs_ref[slot]], axis=0)
        weight = jnp.concatenate(
            [weight_ref[held[side, slot], first:, :] for side in range(2)], axis=0
        )
        mixed += lax.dot_general(
            branch, weight, (((0,), (0,)), ((), ())), preferred_element_type=jnp.float32
        )
    mixed = mixed.astype(jnp.bfloat16)
    out_ref[...] = mixed
    for ref in copies_ref:
        ref[...] = jnp.broadcast_to(mixed[None], ref.shape)


def pack_kernel(value_ref, gate_ref, mix_ref, first_ref, *rest_refs):
    *later_refs, sems = rest_refs
    channels = value_ref.shape[1]
    moves = []
    for layer, rows_ref in enumerate((first_ref.at[0], *later_refs)):
        for k, shard_ref in enumerate((value_ref, gate_ref, mix_ref)):
            target = rows_ref.at[pl.ds(k * channels, channels)]
            moves.append(
                pltpu.make_async_copy(shard_ref.at[layer], target, sems.at[len(moves)])
            )
    for move in moves:
        move.start()
    for move in moves:
        move.wait()
    rows = first_ref[0]
    for at in range(1, first_ref.shape[0]):
        first_ref[at] = rows


def vmem(n):
    return [pl.BlockSpec(memory_space=pltpu.VMEM)] * n


def kernel_call(kernel, out_shape, *operands):
    return pl.pallas_call(
        kernel, out_shape=out_shape, in_specs=vmem(len(operands)), out_specs=vmem(len(out_shape))
    )(*(pltpu.with_memory_space_constraint(a, pltpu.VMEM) for a in operands))


def pack_call(value_proj, gate_proj, mix_proj, count):
    layers, channels, width = value_proj.shape
    rows = (3 * channels, width)
    out = [pltpu.VMEM((count, *rows), value_proj.dtype)]
    out += [pltpu.VMEM(rows, value_proj.dtype)] * (layers - 1)
    return pl.pallas_call(
        pack_kernel,
        out_shape=out,
        in_specs=[pl.BlockSpec(memory_space=pl.ANY)] * 3,
        out_specs=vmem(len(out)),
        scratch_shapes=[pltpu.SemaphoreType.DMA((3 * layers,))],
        name="pack",
    )(value_proj, gate_proj, mix_proj)


def project_call(slotted, hopped, mine, theirs, gains, weights):
    _, tok, _ = mine.shape
    channels = weights.shape[1] // 3
    out = [pltpu.VMEM((channels, n), jnp.bfloat16) for n in (tok, tok, LANES)]
    kernel = functools.partial(project_kernel, slotted, hopped)
    return kernel_call(kernel, out, mine, theirs, gains, weights)


def mix_call(hopped, mine, theirs, weights, residual, copies):
    shape, dtype = residual.shape, jnp.bfloat16
    if copies:
        out = [pltpu.VMEM(shape, dtype), pltpu.VMEM((copies, *shape), dtype)]
    else:
        out = [jax.ShapeDtypeStruct(shape, dtype)]
    kernel = functools.partial(mix_kernel, hopped)
    return kernel_call(kernel, out, mine, theirs, weights, residual)


def scan_call(layer, value, before, consts, maps, offset, count):
    channels, tok = value.shape
    out = [
        pltpu.VMEM((channels, tok), jnp.float32),
        pltpu.VMEM((channels, tok), jnp.float32),
        pltpu.VMEM((count, 1, 2 * channels), jnp.float32),
    ]
    kernel = functools.partial(scan_kernel, layer)
    return kernel_call(kernel, out, value, before, consts, maps, offset)


def close_call(msgs, cum, state, gate, copies):
    out = [pltpu.VMEM((copies, *cum.shape), jnp.bfloat16)]
    return kernel_call(close_kernel, out, msgs, cum, state, gate)[0]


def copy_kernel(in_ref, out_ref):
    out_ref[...] = in_ref[...]


def copy_call(array):
    return kernel_call(copy_kernel, [pltpu.VMEM(array.shape, array.dtype)], array)[0]


def exchange(copies, axis):
    return lax.all_to_all(copies, axis, split_axis=0, concat_axis=0, tiled=True)


def shift(array, axis, steps):
    count = lax.axis_size(axis)
    return lax.ppermute(array, axis, [(i, (i + steps) % count) for i in range(count)])


def far_hop(array, axis, hops=1):
    return shift(array, axis, len(NEAR) * hops)


def near_hops(held, axis):
    count, cores = lax.axis_size(axis), lax.axis_size("core")

    def hop(steps):
        pairs = [
            (i * cores + c, (i + steps * (1 - 2 * c)) % count * cores + c)
            for i in range(count)
            for c in range(cores)
        ]
        return lax.ppermute(held, (axis, "core"), pairs)

    return jnp.concatenate([hop(n) if n else held for n in NEAR])


def local(
    tokens,
    norm_gain,
    value_proj,
    gate_proj,
    conv_taps,
    recur_map,
    input_map,
    decay_param,
    decay_offset,
    mix_proj,
):
    own_cols = tokens.shape[1]
    chips, cores, count = (lax.axis_size(name) for name in ("x", "core", "sp"))

    def swap(array):
        return shift(array, "core", 1)

    first, shard = pack_call(value_proj, gate_proj, mix_proj, count)
    weights = exchange(first, "sp")
    held = jnp.stack([tokens, far_hop(tokens, "x")])
    mine = near_hops(held, "x")
    _, shard = lax.optimization_barrier((mine, shard))
    hop_one = far_hop(shard, "sp")
    rates = -RATE_SCALE * jax.nn.softplus(-decay_param)
    consts = jnp.concatenate([conv_taps.transpose(0, 2, 1), rates[:, :, None]], axis=2)
    consts = jnp.pad(consts, ((0, 0), (0, 0), (0, LANES - consts.shape[2])))
    maps = jnp.concatenate([recur_map[:, 0], input_map[:, 0]], axis=2).transpose(0, 2, 1)
    gains = [gain.reshape(chips * cores, 1, own_cols) for gain in norm_gain]
    gains[1] = copy_call(gains[1])
    gains[1] = copy_call(gains[1])

    residual = tokens
    for layer in range(LAYERS):
        more = layer + 1 < LAYERS
        if layer:
            mine = exchange(copies[0], "x")
            weights = later_weights
        theirs = swap(mine)
        value_rows, gate_rows, tail = project_call(
            layer == 0, layer > 0, mine, theirs, gains[layer], weights
        )
        before = lax.ppermute(tail, "sp", [(i, i + 1) for i in range(count - 1)])
        cum, state, msg = scan_call(layer, value_rows, before, consts, maps, decay_offset, count)
        msgs = exchange(msg, "sp")
        sent = close_call(msgs, cum, state, gate_rows, chips)
        mine = exchange(sent, "x")
        if more:
            _, shard, hop_one = lax.optimization_barrier((sent, shard, hop_one))
            hop_back = far_hop(shard, "sp", -1)
            hop_two = far_hop(hop_one, "sp")
        theirs = swap(mine)
        residual, *copies = mix_call(
            layer > 0, mine, theirs, weights, residual, chips if more else 0
        )
        if more:
            _, *held = lax.optimization_barrier((copies[0], shard, hop_one, hop_two, hop_back))
            later_weights = near_hops(jnp.stack(held), "sp")
    return residual


def solution(mesh):
    grid = mesh.devices
    split = Mesh(grid.reshape(*grid.shape[:2], grid.shape[2] // 2, 2), ("grp", "sp", "x", "core"))
    tp = ("x", "core")
    in_specs = (
        P(("grp", "sp"), tp),
        P(),
        P(None, tp, "sp"),
        P(None, tp, "sp"),
        P(None, None, tp),
        P(None, tp, None, None),
        P(None, tp, None, None),
        P(None, tp),
        P(None, tp, "sp"),
        P(None, "sp", tp),
    )
    return jax.shard_map(
        local, mesh=split, in_specs=in_specs, out_specs=P(("grp", "sp"), tp), check_vma=False
    )
```

```python
import functools

import jax
import jax.numpy as jnp
from jax import lax
from jax.experimental import pallas as pl
from jax.experimental.pallas import tpu as pltpu
from jax.sharding import Mesh, PartitionSpec as P


LAYERS = 2
EPS = 1e-06
RATE_SCALE = 8.0
LANES = 128
NEAR = (-2, -1, 0, 1)


def one_minus_exp(u):
    series = 1.0
    for n in range(9, 1, -1):
        series = 1.0 + u * series * (1.0 / n)
    return jnp.where(u > -0.5, -u * series, 1.0 - jnp.exp(u))


def scan_kernel(
    layer, value_ref, before_ref, consts_ref, maps_ref, offset_ref, cum_ref, state_ref, msg_ref
):
    channels, tok = value_ref.shape
    taps = 4
    value = value_ref[...].astype(jnp.float32)
    full = jnp.concatenate([before_ref[...].astype(jnp.float32), value], axis=1)
    consts = consts_ref[layer]
    smoothed = consts[:, taps - 1 : taps] * value
    for back in range(1, taps):
        shifted = pltpu.roll(full, back, axis=1)[:, LANES:]
        smoothed = smoothed + consts[:, taps - 1 - back : taps - back] * shifted
    half = smoothed.astype(jnp.bfloat16)
    gates = lax.dot_general(
        maps_ref[layer], half, (((1,), (0,)), ((), ())), preferred_element_type=jnp.float32
    )
    gates = 1.0 / (1.0 + jnp.exp(-gates))
    recur, inputs = gates[:channels], gates[channels:]
    log_decay = consts[:, taps : taps + 1] * recur + offset_ref[layer]
    a = jnp.exp(log_decay)
    b = jnp.sqrt(one_minus_exp(2.0 * log_decay)) * inputs * smoothed
    lane = lax.broadcasted_iota(jnp.int32, (channels, tok), 1)
    step = 1
    while step < tok:
        inside = lane >= step
        b = jnp.where(inside, a * pltpu.roll(b, step, axis=1), 0.0) + b
        a = jnp.where(inside, pltpu.roll(a, step, axis=1), 1.0) * a
        step *= 2
    cum_ref[...] = a
    state_ref[...] = b
    last = jnp.concatenate([a[:, tok - LANES :], b[:, tok - LANES :]], axis=0)
    row = last.T[LANES - 1 : LANES, :]
    msg_ref[...] = jnp.broadcast_to(row[None], msg_ref.shape)


def close_kernel(msgs_ref, cum_ref, state_ref, gate_ref, out_ref):
    channels, tok = cum_ref.shape
    count = msgs_ref.shape[0]
    position = lax.axis_index("sp")
    carry = jnp.zeros((1, channels), jnp.float32)
    for s in range(count - 1):
        line = msgs_ref[s]
        step = line[:, :channels] * carry + line[:, channels:]
        carry = jnp.where(s < position, step, carry)
    wide = jnp.broadcast_to(carry, (LANES, channels)).T
    wide = jnp.concatenate([wide] * (tok // LANES), axis=1)
    hidden = state_ref[...] + cum_ref[...] * wide
    gate = gate_ref[...].astype(jnp.float32)
    branch = (hidden * (gate / (1.0 + jnp.exp(-gate)))).astype(jnp.bfloat16)
    out_ref[...] = jnp.broadcast_to(branch[None], out_ref.shape)


def weight_slot(block, count, hopped):
    if not hopped:
        return block
    steps, far = len(NEAR), count // len(NEAR)
    sign = 1 - 2 * lax.axis_index("core")
    at = lax.rem(sign * (lax.axis_index("sp") - block) + 2 * count - NEAR[0], count)
    return lax.rem(at, steps) * far + lax.rem(sign * lax.div(at, steps) + far, far)


def piece_block(side, slot, chips, slotted):
    core, source = lax.axis_index("core"), slot
    core = core if side == 0 else 1 - core
    if slotted:
        far = chips // len(NEAR)
        behind = slot % far * len(NEAR) + (1 - 2 * core) * NEAR[slot // far]
        source = lax.rem(lax.axis_index("x") + 2 * chips - behind, chips)
    return 2 * source + core


def project_kernel(
    slotted, hopped, mine_ref, theirs_ref, gain_ref, weight_ref, value_ref, gate_ref, tail_ref
):
    chips, tok, width = mine_ref.shape
    channels = value_ref.shape[0]
    product = jnp.zeros((2 * channels, tok), jnp.float32)
    squares = jnp.zeros((tok, width), jnp.float32)
    pieces = (mine_ref, theirs_ref)
    for side in range(2):
        for slot in range(chips):
            block = piece_block(side, slot, chips, slotted)
            held = weight_slot(block, weight_ref.shape[0], hopped)
            wide = pieces[side][slot].astype(jnp.float32)
            squares += wide * wide
            scaled = (wide * gain_ref[block]).astype(jnp.bfloat16)
            product += lax.dot_general(
                weight_ref[held, : 2 * channels, :],
                scaled,
                (((1,), (1,)), ((), ())),
                preferred_element_type=jnp.float32,
            )
    mean = jnp.sum(squares.T, axis=0, keepdims=True) * (1.0 / (2 * chips * width))
    rows = (product * lax.rsqrt(mean + EPS)).astype(jnp.bfloat16)
    value_ref[...] = rows[:channels]
    gate_ref[...] = rows[channels:]
    tail_ref[...] = rows[:channels, tok - LANES :]


def mix_kernel(hopped, branch_ref, weight_ref, residual_ref, out_ref, *copies_ref):
    blocks, channels, _ = branch_ref.shape
    count, rows, _ = weight_ref.shape
    mixed = residual_ref[...].astype(jnp.float32)
    for at in range(0, blocks, 2):
        pair = (at, at + 1)
        weight = [weight_ref[weight_slot(b, count, hopped), rows - channels :, :] for b in pair]
        mixed += lax.dot_general(
            jnp.concatenate([branch_ref[b] for b in pair], axis=0),
            jnp.concatenate(weight, axis=0),
            (((0,), (0,)), ((), ())),
            preferred_element_type=jnp.float32,
        )
    mixed = mixed.astype(jnp.bfloat16)
    out_ref[...] = mixed
    for ref in copies_ref:
        ref[...] = jnp.broadcast_to(mixed[None], ref.shape)


def pack_kernel(value_ref, gate_ref, mix_ref, first_ref, *rest_refs):
    *later_refs, sems = rest_refs
    channels = value_ref.shape[1]
    moves = []
    for layer, rows_ref in enumerate((first_ref.at[0], *later_refs)):
        for k, shard_ref in enumerate((value_ref, gate_ref, mix_ref)):
            target = rows_ref.at[pl.ds(k * channels, channels)]
            moves.append(
                pltpu.make_async_copy(shard_ref.at[layer], target, sems.at[len(moves)])
            )
    for move in moves:
        move.start()
    for move in moves:
        move.wait()
    rows = first_ref[0]
    for at in range(1, first_ref.shape[0]):
        first_ref[at] = rows


def vmem(n):
    return [pl.BlockSpec(memory_space=pltpu.VMEM)] * n


def kernel_call(kernel, out_shape, *operands):
    return pl.pallas_call(
        kernel, out_shape=out_shape, in_specs=vmem(len(operands)), out_specs=vmem(len(out_shape))
    )(*(pltpu.with_memory_space_constraint(a, pltpu.VMEM) for a in operands))


def pack_call(value_proj, gate_proj, mix_proj, count):
    layers, channels, width = value_proj.shape
    rows = (3 * channels, width)
    out = [pltpu.VMEM((count, *rows), value_proj.dtype)]
    out += [pltpu.VMEM(rows, value_proj.dtype)] * (layers - 1)
    return pl.pallas_call(
        pack_kernel,
        out_shape=out,
        in_specs=[pl.BlockSpec(memory_space=pl.ANY)] * 3,
        out_specs=vmem(len(out)),
        scratch_shapes=[pltpu.SemaphoreType.DMA((3 * layers,))],
        name="pack",
    )(value_proj, gate_proj, mix_proj)


def project_call(slotted, hopped, mine, theirs, gains, weights):
    _, tok, _ = mine.shape
    channels = weights.shape[1] // 3
    out = [pltpu.VMEM((channels, n), jnp.bfloat16) for n in (tok, tok, LANES)]
    kernel = functools.partial(project_kernel, slotted, hopped)
    return kernel_call(kernel, out, mine, theirs, gains, weights)


def mix_call(hopped, branch, weights, residual, copies):
    shape, dtype = residual.shape, jnp.bfloat16
    if copies:
        out = [pltpu.VMEM(shape, dtype), pltpu.VMEM((copies, *shape), dtype)]
    else:
        out = [jax.ShapeDtypeStruct(shape, dtype)]
    kernel = functools.partial(mix_kernel, hopped)
    return kernel_call(kernel, out, branch, weights, residual)


def scan_call(layer, value, before, consts, maps, offset, count):
    channels, tok = value.shape
    out = [
        pltpu.VMEM((channels, tok), jnp.float32),
        pltpu.VMEM((channels, tok), jnp.float32),
        pltpu.VMEM((count, 1, 2 * channels), jnp.float32),
    ]
    kernel = functools.partial(scan_kernel, layer)
    return kernel_call(kernel, out, value, before, consts, maps, offset)


def close_call(msgs, cum, state, gate, copies):
    out = [pltpu.VMEM((copies, *cum.shape), jnp.bfloat16)]
    return kernel_call(close_kernel, out, msgs, cum, state, gate)[0]


def copy_kernel(in_ref, out_ref):
    out_ref[...] = in_ref[...]


def copy_call(array):
    return kernel_call(copy_kernel, [pltpu.VMEM(array.shape, array.dtype)], array)[0]


def exchange(copies, axis):
    return lax.all_to_all(copies, axis, split_axis=0, concat_axis=0, tiled=True)


def shift(array, axis, steps):
    count = lax.axis_size(axis)
    return lax.ppermute(array, axis, [(i, (i + steps) % count) for i in range(count)])


def far_hop(array, axis, hops=1):
    return shift(array, axis, len(NEAR) * hops)


def near_hops(held, axis):
    count, cores = lax.axis_size(axis), lax.axis_size("core")

    def hop(steps):
        pairs = [
            (i * cores + c, (i + steps * (1 - 2 * c)) % count * cores + c)
            for i in range(count)
            for c in range(cores)
        ]
        return lax.ppermute(held, (axis, "core"), pairs)

    return jnp.concatenate([hop(n) if n else held for n in NEAR])


def local(
    tokens,
    norm_gain,
    value_proj,
    gate_proj,
    conv_taps,
    recur_map,
    input_map,
    decay_param,
    decay_offset,
    mix_proj,
):
    own_cols = tokens.shape[1]
    chips, cores, count = (lax.axis_size(name) for name in ("x", "core", "sp"))

    def swap(array):
        return shift(array, "core", 1)

    first, shard = pack_call(value_proj, gate_proj, mix_proj, count)
    weights = exchange(first, "sp")
    held = jnp.stack([tokens, far_hop(tokens, "x")])
    mine = near_hops(held, "x")
    _, shard = lax.optimization_barrier((mine, shard))
    hop_one = far_hop(shard, "sp")
    rates = -RATE_SCALE * jax.nn.softplus(-decay_param)
    consts = jnp.concatenate([conv_taps.transpose(0, 2, 1), rates[:, :, None]], axis=2)
    consts = jnp.pad(consts, ((0, 0), (0, 0), (0, LANES - consts.shape[2])))
    maps = jnp.concatenate([recur_map[:, 0], input_map[:, 0]], axis=2).transpose(0, 2, 1)
    gains = [gain.reshape(chips * cores, 1, own_cols) for gain in norm_gain]
    gains[1] = copy_call(gains[1])
    gains[1] = copy_call(gains[1])

    residual = tokens
    for layer in range(LAYERS):
        more = layer + 1 < LAYERS
        if layer:
            mine = exchange(copies[0], "x")
            weights = later_weights
        theirs = swap(mine)
        value_rows, gate_rows, tail = project_call(
            layer == 0, layer > 0, mine, theirs, gains[layer], weights
        )
        before = lax.ppermute(tail, "sp", [(i, i + 1) for i in range(count - 1)])
        cum, state, msg = scan_call(layer, value_rows, before, consts, maps, decay_offset, count)
        msgs = exchange(msg, "sp")
        sent = close_call(msgs, cum, state, gate_rows, chips * cores)
        branch = exchange(sent, ("x", "core"))
        if more:
            _, shard, hop_one = lax.optimization_barrier((sent, shard, hop_one))
            hop_back = far_hop(shard, "sp", -1)
            hop_two = far_hop(hop_one, "sp")
        residual, *copies = mix_call(layer > 0, branch, weights, residual, chips if more else 0)
        if more:
            _, *held = lax.optimization_barrier((copies[0], shard, hop_one, hop_two, hop_back))
            later_weights = near_hops(jnp.stack(held), "sp")
    return residual


def solution(mesh):
    grid = mesh.devices
    split = Mesh(grid.reshape(*grid.shape[:2], grid.shape[2] // 2, 2), ("grp", "sp", "x", "core"))
    tp = ("x", "core")
    in_specs = (
        P(("grp", "sp"), tp),
        P(),
        P(None, tp, "sp"),
        P(None, tp, "sp"),
        P(None, None, tp),
        P(None, tp, None, None),
        P(None, tp, None, None),
        P(None, tp),
        P(None, tp, "sp"),
        P(None, "sp", tp),
    )
    return jax.shard_map(
        local, mesh=split, in_specs=in_specs, out_specs=P(("grp", "sp"), tp), check_vma=False
    )
```

```python
import functools

import jax
import jax.numpy as jnp
from jax import lax
from jax.experimental import pallas as pl
from jax.experimental.pallas import tpu as pltpu
from jax.sharding import Mesh, PartitionSpec as P


LAYERS = 2
EPS = 1e-06
RATE_SCALE = 8.0
LANES = 128
NEAR = (-2, -1, 0, 1)


def one_minus_exp(u):
    series = 1.0
    for n in range(9, 1, -1):
        series = 1.0 + u * series * (1.0 / n)
    return jnp.where(u > -0.5, -u * series, 1.0 - jnp.exp(u))


def scan_kernel(
    layer, value_ref, before_ref, consts_ref, maps_ref, offset_ref, cum_ref, state_ref, msg_ref
):
    channels, tok = value_ref.shape
    taps = 4
    value = value_ref[...].astype(jnp.float32)
    full = jnp.concatenate([before_ref[...].astype(jnp.float32), value], axis=1)
    consts = consts_ref[layer]
    smoothed = consts[:, taps - 1 : taps] * value
    for back in range(1, taps):
        shifted = pltpu.roll(full, back, axis=1)[:, LANES:]
        smoothed = smoothed + consts[:, taps - 1 - back : taps - back] * shifted
    half = smoothed.astype(jnp.bfloat16)
    gates = lax.dot_general(
        maps_ref[layer], half, (((1,), (0,)), ((), ())), preferred_element_type=jnp.float32
    )
    gates = 1.0 / (1.0 + jnp.exp(-gates))
    recur, inputs = gates[:channels], gates[channels:]
    log_decay = consts[:, taps : taps + 1] * recur + offset_ref[layer]
    a = jnp.exp(log_decay)
    b = jnp.sqrt(one_minus_exp(2.0 * log_decay)) * inputs * smoothed
    lane = lax.broadcasted_iota(jnp.int32, (channels, tok), 1)
    step = 1
    while step < tok:
        inside = lane >= step
        b = jnp.where(inside, a * pltpu.roll(b, step, axis=1), 0.0) + b
        a = jnp.where(inside, pltpu.roll(a, step, axis=1), 1.0) * a
        step *= 2
    cum_ref[...] = a
    state_ref[...] = b
    last = jnp.concatenate([a[:, tok - LANES :], b[:, tok - LANES :]], axis=0)
    row = last.T[LANES - 1 : LANES, :]
    msg_ref[...] = jnp.broadcast_to(row[None], msg_ref.shape)


def close_kernel(msgs_ref, cum_ref, state_ref, gate_ref, out_ref):
    channels, tok = cum_ref.shape
    count = msgs_ref.shape[0]
    position = lax.axis_index("sp")
    carry = jnp.zeros((1, channels), jnp.float32)
    for s in range(count - 1):
        line = msgs_ref[s]
        step = line[:, :channels] * carry + line[:, channels:]
        carry = jnp.where(s < position, step, carry)
    wide = jnp.broadcast_to(carry, (LANES, channels)).T
    wide = jnp.concatenate([wide] * (tok // LANES), axis=1)
    hidden = state_ref[...] + cum_ref[...] * wide
    gate = gate_ref[...].astype(jnp.float32)
    branch = (hidden * (gate / (1.0 + jnp.exp(-gate)))).astype(jnp.bfloat16)
    out_ref[...] = jnp.broadcast_to(branch[None], out_ref.shape)


def weight_slot(block, count, hopped):
    if not hopped:
        return block
    steps, far = len(NEAR), count // len(NEAR)
    sign = 1 - 2 * lax.axis_index("core")
    at = lax.rem(sign * (lax.axis_index("sp") - block) + 2 * count - NEAR[0], count)
    return lax.rem(at, steps) * far + lax.rem(sign * lax.div(at, steps) + far, far)


def piece_block(side, slot, chips, slotted):
    core, source = lax.axis_index("core"), slot
    core = core if side == 0 else 1 - core
    if slotted:
        far = chips // len(NEAR)
        behind = slot % far * len(NEAR) + (1 - 2 * core) * NEAR[slot // far]
        source = lax.rem(lax.axis_index("x") + 2 * chips - behind, chips)
    return 2 * source + core


def project_kernel(
    slotted, hopped, mine_ref, theirs_ref, gain_ref, weight_ref, value_ref, gate_ref, tail_ref
):
    chips, tok, width = mine_ref.shape
    channels = value_ref.shape[0]
    product = jnp.zeros((2 * channels, tok), jnp.float32)
    squares = jnp.zeros((tok, width), jnp.float32)
    pieces = (mine_ref, theirs_ref)
    for side in range(2):
        for slot in range(chips):
            block = piece_block(side, slot, chips, slotted)
            held = weight_slot(block, weight_ref.shape[0], hopped)
            wide = pieces[side][slot].astype(jnp.float32)
            squares += wide * wide
            scaled = (wide * gain_ref[block]).astype(jnp.bfloat16)
            product += lax.dot_general(
                weight_ref[held, : 2 * channels, :],
                scaled,
                (((1,), (1,)), ((), ())),
                preferred_element_type=jnp.float32,
            )
    mean = jnp.sum(squares.T, axis=0, keepdims=True) * (1.0 / (2 * chips * width))
    rows = (product * lax.rsqrt(mean + EPS)).astype(jnp.bfloat16)
    value_ref[...] = rows[:channels]
    gate_ref[...] = rows[channels:]
    tail_ref[...] = rows[:channels, tok - LANES :]


def mix_kernel(mine_ref, theirs_ref, weight_ref, residual_ref, out_ref, *copies_ref):
    chips, channels, _ = mine_ref.shape
    count, rows, _ = weight_ref.shape
    mixed = residual_ref[...].astype(jnp.float32)
    for slot in range(chips):
        held = [weight_slot(piece_block(side, slot, chips, False), count, True) for side in range(2)]
        branch = jnp.concatenate([mine_ref[slot], theirs_ref[slot]], axis=0)
        weight = jnp.concatenate([weight_ref[at, rows - channels :, :] for at in held], axis=0)
        mixed += lax.dot_general(
            branch, weight, (((0,), (0,)), ((), ())), preferred_element_type=jnp.float32
        )
    mixed = mixed.astype(jnp.bfloat16)
    out_ref[...] = mixed
    for ref in copies_ref:
        ref[...] = jnp.broadcast_to(mixed[None], ref.shape)


def pack_kernel(value_ref, gate_ref, mix_ref, first_ref, later_ref, sems):
    layers, channels, _ = value_ref.shape
    shards = [ref.at[layer] for layer in range(layers) for ref in (value_ref, gate_ref, mix_ref)]
    moves = []
    for k, shard_ref in enumerate(shards):
        rows_ref, at = (first_ref.at[0], k) if k < 2 else (later_ref, k - 2)
        target = rows_ref.at[pl.ds(at * channels, channels)]
        moves.append(pltpu.make_async_copy(shard_ref, target, sems.at[k]))
    for move in moves:
        move.start()
    for move in moves:
        move.wait()
    rows = first_ref[0]
    for at in range(1, first_ref.shape[0]):
        first_ref[at] = rows


def vmem(n):
    return [pl.BlockSpec(memory_space=pltpu.VMEM)] * n


def kernel_call(kernel, out_shape, *operands):
    return pl.pallas_call(
        kernel, out_shape=out_shape, in_specs=vmem(len(operands)), out_specs=vmem(len(out_shape))
    )(*(pltpu.with_memory_space_constraint(a, pltpu.VMEM) for a in operands))


def pack_call(value_proj, gate_proj, mix_proj, count):
    layers, channels, width = value_proj.shape
    dtype = value_proj.dtype
    out = [
        pltpu.VMEM((count, 2 * channels, width), dtype),
        pltpu.VMEM(((3 * layers - 2) * channels, width), dtype),
    ]
    return pl.pallas_call(
        pack_kernel,
        out_shape=out,
        in_specs=[pl.BlockSpec(memory_space=pl.ANY)] * 3,
        out_specs=vmem(len(out)),
        scratch_shapes=[pltpu.SemaphoreType.DMA((3 * layers,))],
        name="pack",
    )(value_proj, gate_proj, mix_proj)


def project_call(slotted, hopped, mine, theirs, gains, weights, channels):
    _, tok, _ = mine.shape
    out = [pltpu.VMEM((channels, n), jnp.bfloat16) for n in (tok, tok, LANES)]
    kernel = functools.partial(project_kernel, slotted, hopped)
    return kernel_call(kernel, out, mine, theirs, gains, weights)


def mix_call(mine, theirs, weights, residual, copies):
    shape, dtype = residual.shape, jnp.bfloat16
    if copies:
        out = [pltpu.VMEM(shape, dtype), pltpu.VMEM((copies, *shape), dtype)]
    else:
        out = [jax.ShapeDtypeStruct(shape, dtype)]
    return kernel_call(mix_kernel, out, mine, theirs, weights, residual)


def scan_call(layer, value, before, consts, maps, offset, count):
    channels, tok = value.shape
    out = [
        pltpu.VMEM((channels, tok), jnp.float32),
        pltpu.VMEM((channels, tok), jnp.float32),
        pltpu.VMEM((count, 1, 2 * channels), jnp.float32),
    ]
    kernel = functools.partial(scan_kernel, layer)
    return kernel_call(kernel, out, value, before, consts, maps, offset)


def close_call(msgs, cum, state, gate, copies):
    out = [pltpu.VMEM((copies, *cum.shape), jnp.bfloat16)]
    return kernel_call(close_kernel, out, msgs, cum, state, gate)[0]


def copy_kernel(in_ref, out_ref):
    out_ref[...] = in_ref[...]


def copy_call(array):
    return kernel_call(copy_kernel, [pltpu.VMEM(array.shape, array.dtype)], array)[0]


def exchange(copies, axis):
    return lax.all_to_all(copies, axis, split_axis=0, concat_axis=0, tiled=True)


def shift(array, axis, steps):
    count = lax.axis_size(axis)
    return lax.ppermute(array, axis, [(i, (i + steps) % count) for i in range(count)])


def far_hop(array, axis, hops=1):
    return shift(array, axis, len(NEAR) * hops)


def near_hops(held, axis):
    count, cores = lax.axis_size(axis), lax.axis_size("core")

    def hop(steps):
        pairs = [
            (i * cores + c, (i + steps * (1 - 2 * c)) % count * cores + c)
            for i in range(count)
            for c in range(cores)
        ]
        return lax.ppermute(held, (axis, "core"), pairs)

    return jnp.concatenate([hop(n) if n else held for n in NEAR])


def local(
    tokens,
    norm_gain,
    value_proj,
    gate_proj,
    conv_taps,
    recur_map,
    input_map,
    decay_param,
    decay_offset,
    mix_proj,
):
    own_cols, channels = tokens.shape[1], value_proj.shape[1]
    chips, cores, count = (lax.axis_size(name) for name in ("x", "core", "sp"))

    def swap(array):
        return shift(array, "core", 1)

    first, shard = pack_call(value_proj, gate_proj, mix_proj, count)
    weights = exchange(first, "sp")
    held = jnp.stack([tokens, far_hop(tokens, "x")])
    hop_one = far_hop(shard, "sp", -1)
    mine = near_hops(held, "x")
    rates = -RATE_SCALE * jax.nn.softplus(-decay_param)
    consts = jnp.concatenate([conv_taps.transpose(0, 2, 1), rates[:, :, None]], axis=2)
    consts = jnp.pad(consts, ((0, 0), (0, 0), (0, LANES - consts.shape[2])))
    maps = jnp.concatenate([recur_map[:, 0], input_map[:, 0]], axis=2).transpose(0, 2, 1)
    gains = [gain.reshape(chips * cores, 1, own_cols) for gain in norm_gain]
    gains[1] = copy_call(gains[1])
    gains[1] = copy_call(gains[1])
    gains[1] = copy_call(gains[1])

    residual = tokens
    for layer in range(LAYERS):
        more = layer + 1 < LAYERS
        if layer:
            mine = exchange(copies[0], "x")
            weights = later_weights
        theirs = swap(mine)
        value_rows, gate_rows, tail = project_call(
            layer == 0, layer > 0, mine, theirs, gains[layer], weights, channels
        )
        before = lax.ppermute(tail, "sp", [(i, i + 1) for i in range(count - 1)])
        cum, state, msg = scan_call(layer, value_rows, before, consts, maps, decay_offset, count)
        msgs = exchange(msg, "sp")
        if more:
            _, shard, hop_one = lax.optimization_barrier((msg, shard, hop_one))
            hop_back = far_hop(shard, "sp")
            hop_two = far_hop(hop_one, "sp", -1)
        sent = close_call(msgs, cum, state, gate_rows, chips)
        mine = exchange(sent, "x")
        if more:
            held = (shard, hop_back, hop_two, hop_one)
            _, *held = lax.optimization_barrier((sent, *held))
            mix_weights = near_hops(jnp.stack([h[:channels] for h in held]), "sp")
        else:
            mix_weights = weights
        theirs = swap(mine)
        residual, *copies = mix_call(mine, theirs, mix_weights, residual, chips if more else 0)
        if more:
            _, *held = lax.optimization_barrier((copies[0], *held))
            later_weights = near_hops(jnp.stack([h[channels:] for h in held]), "sp")
    return residual


def solution(mesh):
    grid = mesh.devices
    split = Mesh(grid.reshape(*grid.shape[:2], grid.shape[2] // 2, 2), ("grp", "sp", "x", "core"))
    tp = ("x", "core")
    in_specs = (
        P(("grp", "sp"), tp),
        P(),
        P(None, tp, "sp"),
        P(None, tp, "sp"),
        P(None, None, tp),
        P(None, tp, None, None),
        P(None, tp, None, None),
        P(None, tp),
        P(None, tp, "sp"),
        P(None, "sp", tp),
    )
    return jax.shard_map(
        local, mesh=split, in_specs=in_specs, out_specs=P(("grp", "sp"), tp), check_vma=False
    )
```

```python
import functools

import jax
import jax.numpy as jnp
from jax import lax
from jax.experimental import pallas as pl
from jax.experimental.pallas import tpu as pltpu
from jax.sharding import Mesh, PartitionSpec as P


LAYERS = 2
EPS = 1e-06
RATE_SCALE = 8.0
LANES = 128
NEAR = (-2, -1, 0, 1)


def one_minus_exp(u):
    series = 1.0
    for n in range(9, 1, -1):
        series = 1.0 + u * series * (1.0 / n)
    return jnp.where(u > -0.5, -u * series, 1.0 - jnp.exp(u))


def softplus(x):
    y = jnp.exp(-jnp.abs(x))
    z = y / (2.0 + y)
    series = jnp.zeros_like(z)
    for n in range(17, 0, -2):
        series = series * (z * z) + 1.0 / n
    return jnp.maximum(x, 0.0) + 2.0 * z * series


def scan_kernel(
    layer,
    value_ref,
    before_ref,
    taps_ref,
    param_ref,
    recur_ref,
    input_ref,
    offset_ref,
    cum_ref,
    state_ref,
    msg_ref,
):
    channels, tok = value_ref.shape
    taps = taps_ref.shape[1]
    rate = -RATE_SCALE * softplus(-param_ref[layer : layer + 1, :])
    rest = jnp.zeros((LANES - taps - 1, channels), jnp.float32)
    consts = jnp.concatenate([taps_ref[layer], rate, rest], axis=0)
    consts = jnp.concatenate([consts, jnp.zeros((LANES, LANES - channels), jnp.float32)], axis=1).T
    consts = consts[:channels]
    maps = jnp.concatenate([recur_ref[layer, 0], input_ref[layer, 0]], axis=1)
    value = value_ref[...].astype(jnp.float32)
    full = jnp.concatenate([before_ref[...].astype(jnp.float32), value], axis=1)
    smoothed = consts[:, taps - 1 : taps] * value
    for back in range(1, taps):
        shifted = pltpu.roll(full, back, axis=1)[:, LANES:]
        smoothed = smoothed + consts[:, taps - 1 - back : taps - back] * shifted
    half = smoothed.astype(jnp.bfloat16)
    gates = lax.dot_general(
        maps, half, (((0,), (0,)), ((), ())), preferred_element_type=jnp.float32
    )
    gates = 1.0 / (1.0 + jnp.exp(-gates))
    recur, inputs = gates[:channels], gates[channels:]
    log_decay = consts[:, taps : taps + 1] * recur + offset_ref[layer]
    a = jnp.exp(log_decay)
    b = jnp.sqrt(one_minus_exp(2.0 * log_decay)) * inputs * smoothed
    lane = lax.broadcasted_iota(jnp.int32, (channels, tok), 1)
    step = 1
    while step < tok:
        inside = lane >= step
        b = jnp.where(inside, a * pltpu.roll(b, step, axis=1), 0.0) + b
        a = jnp.where(inside, pltpu.roll(a, step, axis=1), 1.0) * a
        step *= 2
    cum_ref[...] = a
    state_ref[...] = b
    last = jnp.concatenate([a[:, tok - LANES :], b[:, tok - LANES :]], axis=0)
    row = last.T[LANES - 1 : LANES, :]
    msg_ref[...] = jnp.broadcast_to(row[None], msg_ref.shape)


def close_kernel(msgs_ref, cum_ref, state_ref, gate_ref, out_ref):
    channels, tok = cum_ref.shape
    count = msgs_ref.shape[0]
    position = lax.axis_index("sp")
    carry = jnp.zeros((1, channels), jnp.float32)
    for s in range(count - 1):
        line = msgs_ref[s]
        step = line[:, :channels] * carry + line[:, channels:]
        carry = jnp.where(s < position, step, carry)
    wide = jnp.broadcast_to(carry, (LANES, channels)).T
    wide = jnp.concatenate([wide] * (tok // LANES), axis=1)
    hidden = state_ref[...] + cum_ref[...] * wide
    gate = gate_ref[...].astype(jnp.float32)
    branch = (hidden * (gate / (1.0 + jnp.exp(-gate)))).astype(jnp.bfloat16)
    out_ref[...] = jnp.broadcast_to(branch[None], out_ref.shape)


def weight_slot(block, count, hopped):
    if not hopped:
        return block
    steps, far = len(NEAR), count // len(NEAR)
    sign = 1 - 2 * lax.axis_index("core")
    at = lax.rem(sign * (lax.axis_index("sp") - block) + 2 * count - NEAR[0], count)
    return lax.rem(at, steps) * far + lax.rem(sign * lax.div(at, steps) + far, far)


def piece_block(side, slot, chips, slotted):
    core, source = lax.axis_index("core"), slot
    core = core if side == 0 else 1 - core
    if slotted:
        far = chips // len(NEAR)
        behind = slot % far * len(NEAR) + (1 - 2 * core) * NEAR[slot // far]
        source = lax.rem(lax.axis_index("x") + 2 * chips - behind, chips)
    return 2 * source + core


def project_kernel(
    slotted, hopped, mine_ref, theirs_ref, gain_ref, weight_ref, value_ref, gate_ref, tail_ref
):
    chips, tok, width = mine_ref.shape
    channels = value_ref.shape[0]
    product = jnp.zeros((2 * channels, tok), jnp.float32)
    squares = jnp.zeros((tok, width), jnp.float32)
    pieces = (mine_ref, theirs_ref)
    for side in range(2):
        for slot in range(chips):
            block = piece_block(side, slot, chips, slotted)
            held = weight_slot(block, weight_ref.shape[0], hopped)
            wide = pieces[side][slot].astype(jnp.float32)
            squares += wide * wide
            scaled = (wide * gain_ref[block]).astype(jnp.bfloat16)
            product += lax.dot_general(
                weight_ref[held, : 2 * channels, :],
                scaled,
                (((1,), (1,)), ((), ())),
                preferred_element_type=jnp.float32,
            )
    mean = jnp.sum(squares.T, axis=0, keepdims=True) * (1.0 / (2 * chips * width))
    rows = (product * lax.rsqrt(mean + EPS)).astype(jnp.bfloat16)
    value_ref[...] = rows[:channels]
    gate_ref[...] = rows[channels:]
    tail_ref[...] = rows[:channels, tok - LANES :]


def mix_kernel(mine_ref, theirs_ref, weight_ref, residual_ref, out_ref, *copies_ref):
    chips, channels, _ = mine_ref.shape
    count, rows, _ = weight_ref.shape
    mixed = residual_ref[...].astype(jnp.float32)
    for slot in range(chips):
        held = [weight_slot(piece_block(side, slot, chips, False), count, True) for side in range(2)]
        branch = jnp.concatenate([mine_ref[slot], theirs_ref[slot]], axis=0)
        weight = jnp.concatenate([weight_ref[at, rows - channels :, :] for at in held], axis=0)
        mixed += lax.dot_general(
            branch, weight, (((0,), (0,)), ((), ())), preferred_element_type=jnp.float32
        )
    mixed = mixed.astype(jnp.bfloat16)
    out_ref[...] = mixed
    for ref in copies_ref:
        ref[...] = jnp.broadcast_to(mixed[None], ref.shape)


def pack_kernel(value_ref, gate_ref, mix_ref, first_ref, later_ref, sems):
    layers, channels, _ = value_ref.shape
    shards = [ref.at[layer] for layer in range(layers) for ref in (value_ref, gate_ref, mix_ref)]
    moves = []
    for k, shard_ref in enumerate(shards):
        rows_ref, at = (first_ref.at[0], k) if k < 2 else (later_ref, k - 2)
        target = rows_ref.at[pl.ds(at * channels, channels)]
        moves.append(pltpu.make_async_copy(shard_ref, target, sems.at[k]))
    for move in moves:
        move.start()
    for move in moves:
        move.wait()
    rows = first_ref[0]
    for at in range(1, first_ref.shape[0]):
        first_ref[at] = rows


def vmem(n):
    return [pl.BlockSpec(memory_space=pltpu.VMEM)] * n


def kernel_call(kernel, out_shape, *operands):
    return pl.pallas_call(
        kernel, out_shape=out_shape, in_specs=vmem(len(operands)), out_specs=vmem(len(out_shape))
    )(*(pltpu.with_memory_space_constraint(a, pltpu.VMEM) for a in operands))


def pack_call(value_proj, gate_proj, mix_proj, count):
    layers, channels, width = value_proj.shape
    dtype = value_proj.dtype
    out = [
        pltpu.VMEM((count, 2 * channels, width), dtype),
        pltpu.VMEM(((3 * layers - 2) * channels, width), dtype),
    ]
    return pl.pallas_call(
        pack_kernel,
        out_shape=out,
        in_specs=[pl.BlockSpec(memory_space=pl.ANY)] * 3,
        out_specs=vmem(len(out)),
        scratch_shapes=[pltpu.SemaphoreType.DMA((3 * layers,))],
        name="pack",
    )(value_proj, gate_proj, mix_proj)


def project_call(slotted, hopped, mine, theirs, gains, weights, channels):
    _, tok, _ = mine.shape
    out = [pltpu.VMEM((channels, n), jnp.bfloat16) for n in (tok, tok, LANES)]
    kernel = functools.partial(project_kernel, slotted, hopped)
    return kernel_call(kernel, out, mine, theirs, gains, weights)


def mix_call(mine, theirs, weights, residual, copies):
    shape, dtype = residual.shape, jnp.bfloat16
    if copies:
        out = [pltpu.VMEM(shape, dtype), pltpu.VMEM((copies, *shape), dtype)]
    else:
        out = [jax.ShapeDtypeStruct(shape, dtype)]
    return kernel_call(mix_kernel, out, mine, theirs, weights, residual)


def scan_call(layer, value, before, taps, param, recur_map, input_map, offset, count):
    channels, tok = value.shape
    out = [
        pltpu.VMEM((channels, tok), jnp.float32),
        pltpu.VMEM((channels, tok), jnp.float32),
        pltpu.VMEM((count, 1, 2 * channels), jnp.float32),
    ]
    kernel = functools.partial(scan_kernel, layer)
    operands = (value, before, taps, param, recur_map, input_map, offset)
    return kernel_call(kernel, out, *operands)


def close_call(msgs, cum, state, gate, copies):
    out = [pltpu.VMEM((copies, *cum.shape), jnp.bfloat16)]
    return kernel_call(close_kernel, out, msgs, cum, state, gate)[0]


def copy_kernel(in_ref, out_ref):
    out_ref[...] = in_ref[...]


def copy_call(array):
    return kernel_call(copy_kernel, [pltpu.VMEM(array.shape, array.dtype)], array)[0]


def exchange(copies, axis):
    return lax.all_to_all(copies, axis, split_axis=0, concat_axis=0, tiled=True)


def shift(array, axis, steps):
    count = lax.axis_size(axis)
    return lax.ppermute(array, axis, [(i, (i + steps) % count) for i in range(count)])


def far_hop(array, axis, hops=1):
    return shift(array, axis, len(NEAR) * hops)


def near_hops(held, axis):
    count, cores = lax.axis_size(axis), lax.axis_size("core")

    def hop(steps):
        pairs = [
            (i * cores + c, (i + steps * (1 - 2 * c)) % count * cores + c)
            for i in range(count)
            for c in range(cores)
        ]
        return lax.ppermute(held, (axis, "core"), pairs)

    return jnp.concatenate([hop(n) if n else held for n in NEAR])


def local(
    tokens,
    norm_gain,
    value_proj,
    gate_proj,
    conv_taps,
    recur_map,
    input_map,
    decay_param,
    decay_offset,
    mix_proj,
):
    own_cols, channels = tokens.shape[1], value_proj.shape[1]
    chips, cores, count = (lax.axis_size(name) for name in ("x", "core", "sp"))

    def swap(array):
        return shift(array, "core", 1)

    first, shard = pack_call(value_proj, gate_proj, mix_proj, count)
    weights = exchange(first, "sp")
    held = jnp.stack([tokens, far_hop(tokens, "x")])
    mine = near_hops(held, "x")
    gains = [gain.reshape(chips * cores, 1, own_cols) for gain in norm_gain]
    gains[1] = copy_call(gains[1])
    gains[1] = copy_call(gains[1])
    gains[1] = copy_call(gains[1])

    residual = tokens
    for layer in range(LAYERS):
        more = layer + 1 < LAYERS
        if layer:
            mine = exchange(copies[0], "x")
            weights = later_weights
        theirs = swap(mine)
        value_rows, gate_rows, tail = project_call(
            layer == 0, layer > 0, mine, theirs, gains[layer], weights, channels
        )
        before = lax.ppermute(tail, "sp", [(i, i + 1) for i in range(count - 1)])
        if more:
            _, shard = lax.optimization_barrier((tail, shard))
            hop_one = far_hop(shard, "sp", -1)
        cum, state, msg = scan_call(
            layer,
            value_rows,
            before,
            conv_taps,
            decay_param,
            recur_map,
            input_map,
            decay_offset,
            count,
        )
        msgs = exchange(msg, "sp")
        if more:
            _, shard, hop_one = lax.optimization_barrier((msg, shard, hop_one))
            hop_back = far_hop(shard, "sp")
            hop_two = far_hop(hop_one, "sp", -1)
        sent = close_call(msgs, cum, state, gate_rows, chips)
        mine = exchange(sent, "x")
        if more:
            held = (shard, hop_back, hop_two, hop_one)
            _, *held = lax.optimization_barrier((sent, *held))
            mix_weights = near_hops(jnp.stack([h[:channels] for h in held]), "sp")
        else:
            mix_weights = weights
        theirs = swap(mine)
        residual, *copies = mix_call(mine, theirs, mix_weights, residual, chips if more else 0)
        if more:
            _, *held = lax.optimization_barrier((copies[0], *held))
            later_weights = near_hops(jnp.stack([h[channels:] for h in held]), "sp")
    return residual


def solution(mesh):
    grid = mesh.devices
    split = Mesh(grid.reshape(*grid.shape[:2], grid.shape[2] // 2, 2), ("grp", "sp", "x", "core"))
    tp = ("x", "core")
    in_specs = (
        P(("grp", "sp"), tp),
        P(),
        P(None, tp, "sp"),
        P(None, tp, "sp"),
        P(None, None, tp),
        P(None, tp, None, None),
        P(None, tp, None, None),
        P(None, tp),
        P(None, tp, "sp"),
        P(None, "sp", tp),
    )
    return jax.shard_map(
        local, mesh=split, in_specs=in_specs, out_specs=P(("grp", "sp"), tp), check_vma=False
    )
```

```python
import functools

import jax
import jax.numpy as jnp
from jax import lax
from jax.experimental import pallas as pl
from jax.experimental.pallas import tpu as pltpu
from jax.sharding import Mesh, PartitionSpec as P


LAYERS = 2
EPS = 1e-06
RATE_SCALE = 8.0
LANES = 128
NEAR = (-2, -1, 0, 1)


def one_minus_exp(u):
    series = 1.0
    for n in range(9, 1, -1):
        series = 1.0 + u * series * (1.0 / n)
    return jnp.where(u > -0.5, -u * series, 1.0 - jnp.exp(u))


def softplus(x):
    y = jnp.exp(-jnp.abs(x))
    z = y / (2.0 + y)
    series = jnp.zeros_like(z)
    for n in range(17, 0, -2):
        series = series * (z * z) + 1.0 / n
    return jnp.maximum(x, 0.0) + 2.0 * z * series


def scan_kernel(
    layer,
    value_ref,
    before_ref,
    taps_ref,
    param_ref,
    recur_ref,
    input_ref,
    offset_ref,
    cum_ref,
    state_ref,
    msg_ref,
):
    channels, tok = value_ref.shape
    taps = taps_ref.shape[1]
    rate = -RATE_SCALE * softplus(-param_ref[layer : layer + 1, :])
    rest = jnp.zeros((LANES - taps - 1, channels), jnp.float32)
    consts = jnp.concatenate([taps_ref[layer], rate, rest], axis=0)
    consts = jnp.concatenate([consts, jnp.zeros((LANES, LANES - channels), jnp.float32)], axis=1).T
    consts = consts[:channels]
    maps = jnp.concatenate([recur_ref[layer, 0], input_ref[layer, 0]], axis=1)
    value = value_ref[...].astype(jnp.float32)
    full = jnp.concatenate([before_ref[...].astype(jnp.float32), value], axis=1)
    smoothed = consts[:, taps - 1 : taps] * value
    for back in range(1, taps):
        shifted = pltpu.roll(full, back, axis=1)[:, LANES:]
        smoothed = smoothed + consts[:, taps - 1 - back : taps - back] * shifted
    half = smoothed.astype(jnp.bfloat16)
    gates = lax.dot_general(
        maps, half, (((0,), (0,)), ((), ())), preferred_element_type=jnp.float32
    )
    gates = 1.0 / (1.0 + jnp.exp(-gates))
    recur, inputs = gates[:channels], gates[channels:]
    log_decay = consts[:, taps : taps + 1] * recur + offset_ref[layer]
    a = jnp.exp(log_decay)
    b = jnp.sqrt(one_minus_exp(2.0 * log_decay)) * inputs * smoothed
    lane = lax.broadcasted_iota(jnp.int32, (channels, tok), 1)
    step = 1
    while step < tok:
        inside = lane >= step
        b = jnp.where(inside, a * pltpu.roll(b, step, axis=1), 0.0) + b
        a = jnp.where(inside, pltpu.roll(a, step, axis=1), 1.0) * a
        step *= 2
    cum_ref[...] = a
    state_ref[...] = b
    last = jnp.concatenate([a[:, tok - LANES :], b[:, tok - LANES :]], axis=0)
    row = last.T[LANES - 1 : LANES, :]
    msg_ref[...] = jnp.broadcast_to(row[None], msg_ref.shape)


def close_kernel(msgs_ref, cum_ref, state_ref, gate_ref, out_ref):
    channels, tok = cum_ref.shape
    count = msgs_ref.shape[0]
    position = lax.axis_index("sp")
    carry = jnp.zeros((1, channels), jnp.float32)
    for s in range(count - 1):
        line = msgs_ref[s]
        step = line[:, :channels] * carry + line[:, channels:]
        carry = jnp.where(s < position, step, carry)
    wide = jnp.broadcast_to(carry, (LANES, channels)).T
    wide = jnp.concatenate([wide] * (tok // LANES), axis=1)
    hidden = state_ref[...] + cum_ref[...] * wide
    gate = gate_ref[...].astype(jnp.float32)
    branch = (hidden * (gate / (1.0 + jnp.exp(-gate)))).astype(jnp.bfloat16)
    out_ref[...] = jnp.broadcast_to(branch[None], out_ref.shape)


def weight_slot(block, count, hopped):
    if not hopped:
        return block
    steps, far = len(NEAR), count // len(NEAR)
    sign = 1 - 2 * lax.axis_index("core")
    at = lax.rem(sign * (lax.axis_index("sp") - block) + 2 * count - NEAR[0], count)
    return lax.rem(at, steps) * far + lax.rem(sign * lax.div(at, steps) + far, far)


def piece_block(side, slot, chips, slotted):
    core, source = lax.axis_index("core"), slot
    core = core if side == 0 else 1 - core
    if slotted:
        far = chips // len(NEAR)
        behind = slot % far * len(NEAR) + (1 - 2 * core) * NEAR[slot // far]
        source = lax.rem(lax.axis_index("x") + 2 * chips - behind, chips)
    return 2 * source + core


def project_kernel(
    slotted, hopped, mine_ref, theirs_ref, gain_ref, weight_ref, value_ref, gate_ref, tail_ref
):
    chips, tok, width = mine_ref.shape
    channels = value_ref.shape[0]
    product = jnp.zeros((2 * channels, tok), jnp.float32)
    squares = jnp.zeros((tok, width), jnp.float32)
    pieces = (mine_ref, theirs_ref)
    for side in range(2):
        for slot in range(chips):
            block = piece_block(side, slot, chips, slotted)
            held = weight_slot(block, weight_ref.shape[0], hopped)
            wide = pieces[side][slot].astype(jnp.float32)
            squares += wide * wide
            scaled = (wide * gain_ref[block]).astype(jnp.bfloat16)
            product += lax.dot_general(
                weight_ref[held, : 2 * channels, :],
                scaled,
                (((1,), (1,)), ((), ())),
                preferred_element_type=jnp.float32,
            )
    mean = jnp.sum(squares.T, axis=0, keepdims=True) * (1.0 / (2 * chips * width))
    rows = (product * lax.rsqrt(mean + EPS)).astype(jnp.bfloat16)
    value_ref[...] = rows[:channels]
    gate_ref[...] = rows[channels:]
    tail_ref[...] = rows[:channels, tok - LANES :]


def mix_kernel(mine_ref, theirs_ref, weight_ref, residual_ref, out_ref, *copies_ref):
    chips, channels, _ = mine_ref.shape
    count, rows, _ = weight_ref.shape
    mixed = residual_ref[...].astype(jnp.float32)
    for slot in range(chips):
        held = [weight_slot(piece_block(side, slot, chips, False), count, True) for side in range(2)]
        branch = jnp.concatenate([mine_ref[slot], theirs_ref[slot]], axis=0)
        weight = jnp.concatenate([weight_ref[at, rows - channels :, :] for at in held], axis=0)
        mixed += lax.dot_general(
            branch, weight, (((0,), (0,)), ((), ())), preferred_element_type=jnp.float32
        )
    mixed = mixed.astype(jnp.bfloat16)
    out_ref[...] = mixed
    for ref in copies_ref:
        ref[...] = jnp.broadcast_to(mixed[None], ref.shape)


def pack_kernel(value_ref, gate_ref, mix_ref, first_ref, later_ref, sems):
    layers, channels, _ = value_ref.shape
    shards = [ref.at[layer] for layer in range(layers) for ref in (value_ref, gate_ref, mix_ref)]
    moves = []
    for k, shard_ref in enumerate(shards):
        rows_ref, at = (first_ref.at[0], k) if k < 2 else (later_ref, k - 2)
        target = rows_ref.at[pl.ds(at * channels, channels)]
        moves.append(pltpu.make_async_copy(shard_ref, target, sems.at[k]))
    for move in moves:
        move.start()
    for move in moves:
        move.wait()
    rows = first_ref[0]
    for at in range(1, first_ref.shape[0]):
        first_ref[at] = rows


def vmem(n):
    return [pl.BlockSpec(memory_space=pltpu.VMEM)] * n


def kernel_call(kernel, out_shape, *operands):
    return pl.pallas_call(
        kernel, out_shape=out_shape, in_specs=vmem(len(operands)), out_specs=vmem(len(out_shape))
    )(*(pltpu.with_memory_space_constraint(a, pltpu.VMEM) for a in operands))


def pack_call(value_proj, gate_proj, mix_proj, count):
    layers, channels, width = value_proj.shape
    dtype = value_proj.dtype
    out = [
        pltpu.VMEM((count, 2 * channels, width), dtype),
        pltpu.VMEM(((3 * layers - 2) * channels, width), dtype),
    ]
    return pl.pallas_call(
        pack_kernel,
        out_shape=out,
        in_specs=[pl.BlockSpec(memory_space=pl.ANY)] * 3,
        out_specs=vmem(len(out)),
        scratch_shapes=[pltpu.SemaphoreType.DMA((3 * layers,))],
        name="pack",
    )(value_proj, gate_proj, mix_proj)


def project_call(slotted, hopped, mine, theirs, gains, weights, channels):
    _, tok, _ = mine.shape
    out = [pltpu.VMEM((channels, n), jnp.bfloat16) for n in (tok, tok, LANES)]
    kernel = functools.partial(project_kernel, slotted, hopped)
    return kernel_call(kernel, out, mine, theirs, gains, weights)


def mix_call(mine, theirs, weights, residual, copies):
    shape, dtype = residual.shape, jnp.bfloat16
    if copies:
        out = [pltpu.VMEM(shape, dtype), pltpu.VMEM((copies, *shape), dtype)]
    else:
        out = [jax.ShapeDtypeStruct(shape, dtype)]
    return kernel_call(mix_kernel, out, mine, theirs, weights, residual)


def scan_call(layer, value, before, taps, param, recur_map, input_map, offset, count):
    channels, tok = value.shape
    out = [
        pltpu.VMEM((channels, tok), jnp.float32),
        pltpu.VMEM((channels, tok), jnp.float32),
        pltpu.VMEM((count, 1, 2 * channels), jnp.float32),
    ]
    kernel = functools.partial(scan_kernel, layer)
    operands = (value, before, taps, param, recur_map, input_map, offset)
    return kernel_call(kernel, out, *operands)


def close_call(msgs, cum, state, gate, copies):
    out = [pltpu.VMEM((copies, *cum.shape), jnp.bfloat16)]
    return kernel_call(close_kernel, out, msgs, cum, state, gate)[0]


def copy_kernel(in_ref, out_ref):
    out_ref[...] = in_ref[...]


def copy_call(array):
    return kernel_call(copy_kernel, [pltpu.VMEM(array.shape, array.dtype)], array)[0]


def exchange(copies, axis):
    return lax.all_to_all(copies, axis, split_axis=0, concat_axis=0, tiled=True)


def shift(array, axis, steps):
    count = lax.axis_size(axis)
    return lax.ppermute(array, axis, [(i, (i + steps) % count) for i in range(count)])


def far_hop(array, axis, hops=1):
    return shift(array, axis, len(NEAR) * hops)


def near_hops(held, axis):
    count, cores = lax.axis_size(axis), lax.axis_size("core")

    def hop(steps):
        pairs = [
            (i * cores + c, (i + steps * (1 - 2 * c)) % count * cores + c)
            for i in range(count)
            for c in range(cores)
        ]
        return lax.ppermute(held, (axis, "core"), pairs)

    return jnp.concatenate([hop(n) if n else held for n in NEAR])


def local(
    tokens,
    norm_gain,
    value_proj,
    gate_proj,
    conv_taps,
    recur_map,
    input_map,
    decay_param,
    decay_offset,
    mix_proj,
):
    own_cols, channels = tokens.shape[1], value_proj.shape[1]
    chips, cores, count = (lax.axis_size(name) for name in ("x", "core", "sp"))

    def swap(array):
        return shift(array, "core", 1)

    far_tokens = far_hop(tokens, "x")
    first, shard = pack_call(value_proj, gate_proj, mix_proj, count)
    weights = exchange(first, "sp")
    mine = near_hops(jnp.stack([tokens, far_tokens]), "x")
    _, shard = lax.optimization_barrier((mine, shard))
    hop_one = far_hop(shard, "sp", -1)
    gains = [gain.reshape(chips * cores, 1, own_cols) for gain in norm_gain]
    gains[1] = copy_call(gains[1])
    gains[1] = copy_call(gains[1])
    gains[1] = copy_call(gains[1])

    residual = tokens
    for layer in range(LAYERS):
        more = layer + 1 < LAYERS
        if layer:
            mine = exchange(copies[0], "x")
            weights = later_weights
        theirs = swap(mine)
        value_rows, gate_rows, tail = project_call(
            layer == 0, layer > 0, mine, theirs, gains[layer], weights, channels
        )
        before = lax.ppermute(tail, "sp", [(i, i + 1) for i in range(count - 1)])
        cum, state, msg = scan_call(
            layer,
            value_rows,
            before,
            conv_taps,
            decay_param,
            recur_map,
            input_map,
            decay_offset,
            count,
        )
        msgs = exchange(msg, "sp")
        if more:
            _, shard, hop_one = lax.optimization_barrier((msg, shard, hop_one))
            hop_back = far_hop(shard, "sp")
            hop_two = far_hop(hop_one, "sp", -1)
        sent = close_call(msgs, cum, state, gate_rows, chips)
        mine = exchange(sent, "x")
        if more:
            held = (shard, hop_back, hop_two, hop_one)
            _, *held = lax.optimization_barrier((sent, *held))
            mix_weights = near_hops(jnp.stack([h[:channels] for h in held]), "sp")
        else:
            mix_weights = weights
        theirs = swap(mine)
        residual, *copies = mix_call(mine, theirs, mix_weights, residual, chips if more else 0)
        if more:
            _, *held = lax.optimization_barrier((copies[0], *held))
            later_weights = near_hops(jnp.stack([h[channels:] for h in held]), "sp")
    return residual


def solution(mesh):
    grid = mesh.devices
    split = Mesh(grid.reshape(*grid.shape[:2], grid.shape[2] // 2, 2), ("grp", "sp", "x", "core"))
    tp = ("x", "core")
    in_specs = (
        P(("grp", "sp"), tp),
        P(),
        P(None, tp, "sp"),
        P(None, tp, "sp"),
        P(None, None, tp),
        P(None, tp, None, None),
        P(None, tp, None, None),
        P(None, tp),
        P(None, tp, "sp"),
        P(None, "sp", tp),
    )
    return jax.shard_map(
        local, mesh=split, in_specs=in_specs, out_specs=P(("grp", "sp"), tp), check_vma=False
    )
```

```python
import functools

import jax
import jax.numpy as jnp
from jax import lax
from jax.experimental import pallas as pl
from jax.experimental.pallas import tpu as pltpu
from jax.sharding import Mesh, PartitionSpec as P


LAYERS = 2
EPS = 1e-06
RATE_SCALE = 8.0
LANES = 128
HALO = 16
NEAR = (-2, -1, 0, 1)


def one_minus_exp(u):
    series = 1.0
    for n in range(9, 1, -1):
        series = 1.0 + u * series * (1.0 / n)
    return jnp.where(u > -0.5, -u * series, 1.0 - jnp.exp(u))


def softplus(x):
    y = jnp.exp(-jnp.abs(x))
    z = y / (2.0 + y)
    series = jnp.zeros_like(z)
    for n in range(17, 0, -2):
        series = series * (z * z) + 1.0 / n
    return jnp.maximum(x, 0.0) + 2.0 * z * series


def scan_kernel(
    layer,
    value_ref,
    before_ref,
    taps_ref,
    param_ref,
    recur_ref,
    input_ref,
    offset_ref,
    cum_ref,
    state_ref,
    msg_ref,
):
    channels, tok = value_ref.shape
    taps = taps_ref.shape[1]
    rate = -RATE_SCALE * softplus(-param_ref[layer : layer + 1, :])
    rest = jnp.zeros((LANES - taps - 1, channels), jnp.float32)
    consts = jnp.concatenate([taps_ref[layer], rate, rest], axis=0)
    consts = jnp.concatenate([consts, jnp.zeros((LANES, LANES - channels), jnp.float32)], axis=1).T
    consts = consts[:channels]
    maps = jnp.concatenate([recur_ref[layer, 0], input_ref[layer, 0]], axis=1)
    value = value_ref[...].astype(jnp.float32)
    full = jnp.concatenate([before_ref[...].astype(jnp.float32), value], axis=1)
    smoothed = consts[:, taps - 1 : taps] * value
    for back in range(1, taps):
        shifted = pltpu.roll(full, back, axis=1)[:, LANES:]
        smoothed = smoothed + consts[:, taps - 1 - back : taps - back] * shifted
    half = smoothed.astype(jnp.bfloat16)
    gates = lax.dot_general(
        maps, half, (((0,), (0,)), ((), ())), preferred_element_type=jnp.float32
    )
    gates = 1.0 / (1.0 + jnp.exp(-gates))
    recur, inputs = gates[:channels], gates[channels:]
    log_decay = consts[:, taps : taps + 1] * recur + offset_ref[layer]
    a = jnp.exp(log_decay)
    b = jnp.sqrt(one_minus_exp(2.0 * log_decay)) * inputs * smoothed
    lane = lax.broadcasted_iota(jnp.int32, (channels, tok), 1)
    step = 1
    while step < tok:
        inside = lane >= step
        b = jnp.where(inside, a * pltpu.roll(b, step, axis=1), 0.0) + b
        a = jnp.where(inside, pltpu.roll(a, step, axis=1), 1.0) * a
        step *= 2
    cum_ref[...] = a
    state_ref[...] = b
    last = jnp.concatenate([a[:, tok - LANES :], b[:, tok - LANES :]], axis=0)
    row = last.T[LANES - 1 : LANES, :]
    msg_ref[...] = jnp.broadcast_to(row[None], msg_ref.shape)


def close_kernel(msgs_ref, cum_ref, state_ref, gate_ref, out_ref):
    channels, tok = cum_ref.shape
    count = msgs_ref.shape[0]
    position = lax.axis_index("sp")
    carry = jnp.zeros((1, channels), jnp.float32)
    for s in range(count - 1):
        line = msgs_ref[s]
        step = line[:, :channels] * carry + line[:, channels:]
        carry = jnp.where(s < position, step, carry)
    wide = jnp.broadcast_to(carry, (LANES, channels)).T
    wide = jnp.concatenate([wide] * (tok // LANES), axis=1)
    hidden = state_ref[...] + cum_ref[...] * wide
    gate = gate_ref[...].astype(jnp.float32)
    branch = (hidden * (gate / (1.0 + jnp.exp(-gate)))).astype(jnp.bfloat16)
    out_ref[...] = jnp.broadcast_to(branch[None], out_ref.shape)


def weight_slot(block, count, hopped):
    if not hopped:
        return block
    steps, far = len(NEAR), count // len(NEAR)
    sign = 1 - 2 * lax.axis_index("core")
    at = lax.rem(sign * (lax.axis_index("sp") - block) + 2 * count - NEAR[0], count)
    return lax.rem(at, steps) * far + lax.rem(sign * lax.div(at, steps) + far, far)


def piece_block(side, slot, chips, slotted):
    core, source = lax.axis_index("core"), slot
    core = core if side == 0 else 1 - core
    if slotted:
        far = chips // len(NEAR)
        behind = slot % far * len(NEAR) + (1 - 2 * core) * NEAR[slot // far]
        source = lax.rem(lax.axis_index("x") + 2 * chips - behind, chips)
    return 2 * source + core


def project_kernel(
    slotted, hopped, mine_ref, theirs_ref, gain_ref, weight_ref, value_ref, gate_ref, edge_ref
):
    chips, held_rows, width = mine_ref.shape
    channels, tok = value_ref.shape
    extra = held_rows - tok
    pieces = (mine_ref, theirs_ref)

    def project(rows_of, count):
        product = jnp.zeros((2 * channels, count), jnp.float32)
        squares = jnp.zeros((count, width), jnp.float32)
        for side in range(2):
            for slot in range(chips):
                block = piece_block(side, slot, chips, slotted)
                held = weight_slot(block, weight_ref.shape[0], hopped)
                wide = rows_of(pieces[side], slot).astype(jnp.float32)
                squares += wide * wide
                scaled = (wide * gain_ref[block]).astype(jnp.bfloat16)
                product += lax.dot_general(
                    weight_ref[held, : 2 * channels, :],
                    scaled,
                    (((1,), (1,)), ((), ())),
                    preferred_element_type=jnp.float32,
                )
        mean = jnp.sum(squares.T, axis=0, keepdims=True) * (1.0 / (2 * chips * width))
        return (product * lax.rsqrt(mean + EPS)).astype(jnp.bfloat16)

    rows = project(lambda ref, slot: ref[slot, extra:, :], tok)
    value_ref[...] = rows[:channels]
    gate_ref[...] = rows[channels:]
    if extra:
        blank = jnp.zeros((LANES - extra, width), jnp.bfloat16)
        edge = project(
            lambda ref, slot: jnp.concatenate([blank, ref[slot, :extra, :]], axis=0), LANES
        )
        edge_ref[...] = edge[:channels]
    else:
        edge_ref[...] = rows[:channels, tok - LANES :]


def mix_kernel(mine_ref, theirs_ref, weight_ref, residual_ref, out_ref, *copies_ref):
    chips, channels, _ = mine_ref.shape
    count, rows, _ = weight_ref.shape
    mixed = residual_ref[...].astype(jnp.float32)
    for slot in range(chips):
        held = [weight_slot(piece_block(side, slot, chips, False), count, True) for side in range(2)]
        branch = jnp.concatenate([mine_ref[slot], theirs_ref[slot]], axis=0)
        weight = jnp.concatenate([weight_ref[at, rows - channels :, :] for at in held], axis=0)
        mixed += lax.dot_general(
            branch, weight, (((0,), (0,)), ((), ())), preferred_element_type=jnp.float32
        )
    mixed = mixed.astype(jnp.bfloat16)
    out_ref[...] = mixed
    for ref in copies_ref:
        ref[...] = jnp.broadcast_to(mixed[None], ref.shape)


def pack_kernel(value_ref, gate_ref, mix_ref, tokens_ref, first_ref, later_ref, last_ref, sems):
    layers, channels, _ = value_ref.shape
    shards = [ref.at[layer] for layer in range(layers) for ref in (value_ref, gate_ref, mix_ref)]
    moves = []
    for k, shard_ref in enumerate(shards):
        rows_ref, at = (first_ref.at[0], k) if k < 2 else (later_ref, k - 2)
        target = rows_ref.at[pl.ds(at * channels, channels)]
        moves.append(pltpu.make_async_copy(shard_ref, target, sems.at[k]))
    last = last_ref.shape[0]
    source = tokens_ref.at[pl.ds(tokens_ref.shape[0] - last, last)]
    moves.append(pltpu.make_async_copy(source, last_ref, sems.at[len(shards)]))
    for move in moves:
        move.start()
    for move in moves:
        move.wait()
    rows = first_ref[0]
    for at in range(1, first_ref.shape[0]):
        first_ref[at] = rows


def vmem(n):
    return [pl.BlockSpec(memory_space=pltpu.VMEM)] * n


def kernel_call(kernel, out_shape, *operands):
    return pl.pallas_call(
        kernel, out_shape=out_shape, in_specs=vmem(len(operands)), out_specs=vmem(len(out_shape))
    )(*(pltpu.with_memory_space_constraint(a, pltpu.VMEM) for a in operands))


def pack_call(value_proj, gate_proj, mix_proj, tokens, count):
    layers, channels, width = value_proj.shape
    dtype = value_proj.dtype
    out = [
        pltpu.VMEM((count, 2 * channels, width), dtype),
        pltpu.VMEM(((3 * layers - 2) * channels, width), dtype),
        pltpu.VMEM((HALO, tokens.shape[1]), tokens.dtype),
    ]
    return pl.pallas_call(
        pack_kernel,
        out_shape=out,
        in_specs=[pl.BlockSpec(memory_space=pl.ANY)] * 4,
        out_specs=vmem(len(out)),
        scratch_shapes=[pltpu.SemaphoreType.DMA((3 * layers + 1,))],
        name="pack",
    )(value_proj, gate_proj, mix_proj, tokens)


def project_call(slotted, hopped, mine, theirs, gains, weights, channels, tok):
    out = [pltpu.VMEM((channels, n), jnp.bfloat16) for n in (tok, tok, LANES)]
    kernel = functools.partial(project_kernel, slotted, hopped)
    return kernel_call(kernel, out, mine, theirs, gains, weights)


def mix_call(mine, theirs, weights, residual, copies):
    shape, dtype = residual.shape, jnp.bfloat16
    if copies:
        out = [pltpu.VMEM(shape, dtype), pltpu.VMEM((copies, *shape), dtype)]
    else:
        out = [jax.ShapeDtypeStruct(shape, dtype)]
    return kernel_call(mix_kernel, out, mine, theirs, weights, residual)


def scan_call(layer, value, before, taps, param, recur_map, input_map, offset, count):
    channels, tok = value.shape
    out = [
        pltpu.VMEM((channels, tok), jnp.float32),
        pltpu.VMEM((channels, tok), jnp.float32),
        pltpu.VMEM((count, 1, 2 * channels), jnp.float32),
    ]
    kernel = functools.partial(scan_kernel, layer)
    operands = (value, before, taps, param, recur_map, input_map, offset)
    return kernel_call(kernel, out, *operands)


def close_call(msgs, cum, state, gate, copies):
    out = [pltpu.VMEM((copies, *cum.shape), jnp.bfloat16)]
    return kernel_call(close_kernel, out, msgs, cum, state, gate)[0]


def copy_kernel(in_ref, out_ref):
    out_ref[...] = in_ref[...]


def copy_call(array):
    return kernel_call(copy_kernel, [pltpu.VMEM(array.shape, array.dtype)], array)[0]


def exchange(copies, axis):
    return lax.all_to_all(copies, axis, split_axis=0, concat_axis=0, tiled=True)


def shift(array, axis, steps):
    count = lax.axis_size(axis)
    return lax.ppermute(array, axis, [(i, (i + steps) % count) for i in range(count)])


def far_hop(array, axis, hops=1):
    return shift(array, axis, len(NEAR) * hops)


def near_hops(held, axis):
    count, cores = lax.axis_size(axis), lax.axis_size("core")

    def hop(steps):
        pairs = [
            (i * cores + c, (i + steps * (1 - 2 * c)) % count * cores + c)
            for i in range(count)
            for c in range(cores)
        ]
        return lax.ppermute(held, (axis, "core"), pairs)

    return jnp.concatenate([hop(n) if n else held for n in NEAR])


def local(
    tokens,
    norm_gain,
    value_proj,
    gate_proj,
    conv_taps,
    recur_map,
    input_map,
    decay_param,
    decay_offset,
    mix_proj,
):
    (tok_rows, own_cols), channels = tokens.shape, value_proj.shape[1]
    chips, cores, count = (lax.axis_size(name) for name in ("x", "core", "sp"))

    def swap(array):
        return shift(array, "core", 1)

    def to_next(array):
        return lax.ppermute(array, "sp", [(i, i + 1) for i in range(count - 1)])

    first, shard, last = pack_call(value_proj, gate_proj, mix_proj, tokens, count)
    last = to_next(last)
    weights = exchange(first, "sp")
    held = jnp.concatenate([last, tokens], axis=0)
    held = jnp.stack([held, far_hop(held, "x")])
    hop_one = far_hop(shard, "sp", -1)
    mine = near_hops(held, "x")
    gains = [gain.reshape(chips * cores, 1, own_cols) for gain in norm_gain]
    gains[1] = copy_call(gains[1])
    gains[1] = copy_call(gains[1])
    gains[1] = copy_call(gains[1])

    residual = tokens
    for layer in range(LAYERS):
        more = layer + 1 < LAYERS
        if layer:
            mine = exchange(copies[0], "x")
            weights = later_weights
        theirs = swap(mine)
        value_rows, gate_rows, edge = project_call(
            layer == 0, layer > 0, mine, theirs, gains[layer], weights, channels, tok_rows
        )
        if layer:
            edge = to_next(edge)
        cum, state, msg = scan_call(
            layer,
            value_rows,
            edge,
            conv_taps,
            decay_param,
            recur_map,
            input_map,
            decay_offset,
            count,
        )
        msgs = exchange(msg, "sp")
        if more:
            _, shard, hop_one = lax.optimization_barrier((msg, shard, hop_one))
            hop_back = far_hop(shard, "sp")
            hop_two = far_hop(hop_one, "sp", -1)
        sent = close_call(msgs, cum, state, gate_rows, chips)
        mine = exchange(sent, "x")
        if more:
            held = (shard, hop_back, hop_two, hop_one)
            _, *held = lax.optimization_barrier((sent, *held))
            mix_weights = near_hops(jnp.stack([h[:channels] for h in held]), "sp")
        else:
            mix_weights = weights
        theirs = swap(mine)
        residual, *copies = mix_call(mine, theirs, mix_weights, residual, chips if more else 0)
        if more:
            _, *held = lax.optimization_barrier((copies[0], *held))
            later_weights = near_hops(jnp.stack([h[channels:] for h in held]), "sp")
    return residual


def solution(mesh):
    grid = mesh.devices
    split = Mesh(grid.reshape(*grid.shape[:2], grid.shape[2] // 2, 2), ("grp", "sp", "x", "core"))
    tp = ("x", "core")
    in_specs = (
        P(("grp", "sp"), tp),
        P(),
        P(None, tp, "sp"),
        P(None, tp, "sp"),
        P(None, None, tp),
        P(None, tp, None, None),
        P(None, tp, None, None),
        P(None, tp),
        P(None, tp, "sp"),
        P(None, "sp", tp),
    )
    return jax.shard_map(
        local, mesh=split, in_specs=in_specs, out_specs=P(("grp", "sp"), tp), check_vma=False
    )
```

```python
import functools

import jax
import jax.numpy as jnp
from jax import lax
from jax.experimental import pallas as pl
from jax.experimental.pallas import tpu as pltpu
from jax.sharding import Mesh, PartitionSpec as P


LAYERS = 2
EPS = 1e-06
RATE_SCALE = 8.0
LANES = 128
NEAR = (-2, -1, 0, 1)


def one_minus_exp(u):
    series = 1.0
    for n in range(9, 1, -1):
        series = 1.0 + u * series * (1.0 / n)
    return jnp.where(u > -0.5, -u * series, 1.0 - jnp.exp(u))


def softplus(x):
    y = jnp.exp(-jnp.abs(x))
    z = y / (2.0 + y)
    series = jnp.zeros_like(z)
    for n in range(17, 0, -2):
        series = series * (z * z) + 1.0 / n
    return jnp.maximum(x, 0.0) + 2.0 * z * series


def scan_kernel(
    layer,
    value_ref,
    before_ref,
    taps_ref,
    param_ref,
    recur_ref,
    input_ref,
    offset_ref,
    cum_ref,
    state_ref,
    msg_ref,
):
    channels, tok = value_ref.shape
    taps = taps_ref.shape[1]
    rate = -RATE_SCALE * softplus(-param_ref[layer : layer + 1, :])
    rest = jnp.zeros((LANES - taps - 1, channels), jnp.float32)
    consts = jnp.concatenate([taps_ref[layer], rate, rest], axis=0)
    consts = jnp.concatenate([consts, jnp.zeros((LANES, LANES - channels), jnp.float32)], axis=1).T
    consts = consts[:channels]
    maps = jnp.concatenate([recur_ref[layer, 0], input_ref[layer, 0]], axis=1)
    value = value_ref[...].astype(jnp.float32)
    full = jnp.concatenate([before_ref[...].astype(jnp.float32), value], axis=1)
    smoothed = consts[:, taps - 1 : taps] * value
    for back in range(1, taps):
        shifted = pltpu.roll(full, back, axis=1)[:, LANES:]
        smoothed = smoothed + consts[:, taps - 1 - back : taps - back] * shifted
    half = smoothed.astype(jnp.bfloat16)
    gates = lax.dot_general(
        maps, half, (((0,), (0,)), ((), ())), preferred_element_type=jnp.float32
    )
    gates = 1.0 / (1.0 + jnp.exp(-gates))
    recur, inputs = gates[:channels], gates[channels:]
    log_decay = consts[:, taps : taps + 1] * recur + offset_ref[layer]
    a = jnp.exp(log_decay)
    b = jnp.sqrt(one_minus_exp(2.0 * log_decay)) * inputs * smoothed
    lane = lax.broadcasted_iota(jnp.int32, (channels, tok), 1)
    step = 1
    while step < tok:
        inside = lane >= step
        b = jnp.where(inside, a * pltpu.roll(b, step, axis=1), 0.0) + b
        a = jnp.where(inside, pltpu.roll(a, step, axis=1), 1.0) * a
        step *= 2
    cum_ref[...] = a
    state_ref[...] = b
    last = jnp.concatenate([a[:, tok - LANES :], b[:, tok - LANES :]], axis=0)
    row = last.T[LANES - 1 : LANES, :]
    msg_ref[...] = jnp.broadcast_to(row[None], msg_ref.shape)


def close_kernel(msgs_ref, cum_ref, state_ref, gate_ref, out_ref):
    channels, tok = cum_ref.shape
    count = msgs_ref.shape[0]
    position = lax.axis_index("sp")
    carry = jnp.zeros((1, channels), jnp.float32)
    for s in range(count - 1):
        line = msgs_ref[s]
        step = line[:, :channels] * carry + line[:, channels:]
        carry = jnp.where(s < position, step, carry)
    wide = jnp.broadcast_to(carry, (LANES, channels)).T
    wide = jnp.concatenate([wide] * (tok // LANES), axis=1)
    hidden = state_ref[...] + cum_ref[...] * wide
    gate = gate_ref[...].astype(jnp.float32)
    branch = (hidden * (gate / (1.0 + jnp.exp(-gate)))).astype(jnp.bfloat16)
    out_ref[...] = jnp.broadcast_to(branch[None], out_ref.shape)


def weight_slot(block, count, hopped):
    if not hopped:
        return block
    steps, far = len(NEAR), count // len(NEAR)
    sign = 1 - 2 * lax.axis_index("core")
    at = lax.rem(sign * (lax.axis_index("sp") - block) + 2 * count - NEAR[0], count)
    return lax.rem(at, steps) * far + lax.rem(sign * lax.div(at, steps) + far, far)


def piece_block(side, slot, chips, slotted):
    core, source = lax.axis_index("core"), slot
    core = core if side == 0 else 1 - core
    if slotted:
        far = chips // len(NEAR)
        behind = slot % far * len(NEAR) + (1 - 2 * core) * NEAR[slot // far]
        source = lax.rem(lax.axis_index("x") + 2 * chips - behind, chips)
    return 2 * source + core


def project_kernel(
    slotted, hopped, mine_ref, theirs_ref, gain_ref, weight_ref, value_ref, gate_ref, tail_ref
):
    chips, tok, width = mine_ref.shape
    channels = value_ref.shape[0]
    product = jnp.zeros((2 * channels, tok), jnp.float32)
    squares = jnp.zeros((tok, width), jnp.float32)
    pieces = (mine_ref, theirs_ref)
    for side in range(2):
        for slot in range(chips):
            block = piece_block(side, slot, chips, slotted)
            held = weight_slot(block, weight_ref.shape[0], hopped)
            wide = pieces[side][slot].astype(jnp.float32)
            squares += wide * wide
            scaled = (wide * gain_ref[block]).astype(jnp.bfloat16)
            product += lax.dot_general(
                weight_ref[held, : 2 * channels, :],
                scaled,
                (((1,), (1,)), ((), ())),
                preferred_element_type=jnp.float32,
            )
    mean = jnp.sum(squares.T, axis=0, keepdims=True) * (1.0 / (2 * chips * width))
    rows = (product * lax.rsqrt(mean + EPS)).astype(jnp.bfloat16)
    value_ref[...] = rows[:channels]
    gate_ref[...] = rows[channels:]
    tail_ref[...] = rows[:channels, tok - LANES :]


def mix_kernel(mine_ref, theirs_ref, weight_ref, residual_ref, out_ref, *copies_ref):
    chips, channels, _ = mine_ref.shape
    count, rows, _ = weight_ref.shape
    mixed = residual_ref[...].astype(jnp.float32)
    for slot in range(chips):
        held = [weight_slot(piece_block(side, slot, chips, False), count, True) for side in range(2)]
        branch = jnp.concatenate([mine_ref[slot], theirs_ref[slot]], axis=0)
        weight = jnp.concatenate([weight_ref[at, rows - channels :, :] for at in held], axis=0)
        mixed += lax.dot_general(
            branch, weight, (((0,), (0,)), ((), ())), preferred_element_type=jnp.float32
        )
    mixed = mixed.astype(jnp.bfloat16)
    out_ref[...] = mixed
    for ref in copies_ref:
        ref[...] = jnp.broadcast_to(mixed[None], ref.shape)


def pack_kernel(value_ref, gate_ref, mix_ref, first_ref, later_ref, sems):
    layers, channels, _ = value_ref.shape
    shards = [ref.at[layer] for layer in range(layers) for ref in (value_ref, gate_ref, mix_ref)]
    moves = []
    for k, shard_ref in enumerate(shards):
        rows_ref, at = (first_ref.at[0], k) if k < 2 else (later_ref, k - 2)
        target = rows_ref.at[pl.ds(at * channels, channels)]
        moves.append(pltpu.make_async_copy(shard_ref, target, sems.at[k]))
    for move in moves:
        move.start()
    for move in moves:
        move.wait()
    rows = first_ref[0]
    for at in range(1, first_ref.shape[0]):
        first_ref[at] = rows


def vmem(n):
    return [pl.BlockSpec(memory_space=pltpu.VMEM)] * n


def kernel_call(kernel, out_shape, *operands):
    return pl.pallas_call(
        kernel, out_shape=out_shape, in_specs=vmem(len(operands)), out_specs=vmem(len(out_shape))
    )(*(pltpu.with_memory_space_constraint(a, pltpu.VMEM) for a in operands))


def pack_call(value_proj, gate_proj, mix_proj, count):
    layers, channels, width = value_proj.shape
    dtype = value_proj.dtype
    out = [
        pltpu.VMEM((count, 2 * channels, width), dtype),
        pltpu.VMEM(((3 * layers - 2) * channels, width), dtype),
    ]
    return pl.pallas_call(
        pack_kernel,
        out_shape=out,
        in_specs=[pl.BlockSpec(memory_space=pl.ANY)] * 3,
        out_specs=vmem(len(out)),
        scratch_shapes=[pltpu.SemaphoreType.DMA((3 * layers,))],
        name="pack",
    )(value_proj, gate_proj, mix_proj)


def project_call(slotted, hopped, mine, theirs, gains, weights, channels):
    _, tok, _ = mine.shape
    out = [pltpu.VMEM((channels, n), jnp.bfloat16) for n in (tok, tok, LANES)]
    kernel = functools.partial(project_kernel, slotted, hopped)
    return kernel_call(kernel, out, mine, theirs, gains, weights)


def mix_call(mine, theirs, weights, residual, copies):
    shape, dtype = residual.shape, jnp.bfloat16
    if copies:
        out = [pltpu.VMEM(shape, dtype), pltpu.VMEM((copies, *shape), dtype)]
    else:
        out = [jax.ShapeDtypeStruct(shape, dtype)]
    return kernel_call(mix_kernel, out, mine, theirs, weights, residual)


def scan_call(layer, value, before, taps, param, recur_map, input_map, offset, count):
    channels, tok = value.shape
    out = [
        pltpu.VMEM((channels, tok), jnp.float32),
        pltpu.VMEM((channels, tok), jnp.float32),
        pltpu.VMEM((count, 1, 2 * channels), jnp.float32),
    ]
    kernel = functools.partial(scan_kernel, layer)
    operands = (value, before, taps, param, recur_map, input_map, offset)
    return kernel_call(kernel, out, *operands)


def close_call(msgs, cum, state, gate, copies):
    out = [pltpu.VMEM((copies, *cum.shape), jnp.bfloat16)]
    return kernel_call(close_kernel, out, msgs, cum, state, gate)[0]


def copy_kernel(in_ref, out_ref):
    out_ref[...] = in_ref[...]


def copy_call(array):
    return kernel_call(copy_kernel, [pltpu.VMEM(array.shape, array.dtype)], array)[0]


def exchange(copies, axis):
    return lax.all_to_all(copies, axis, split_axis=0, concat_axis=0, tiled=True)


def shift(array, axis, steps):
    count = lax.axis_size(axis)
    return lax.ppermute(array, axis, [(i, (i + steps) % count) for i in range(count)])


def far_hop(array, axis, hops=1):
    return shift(array, axis, len(NEAR) * hops)


def near_hops(held, axis):
    count, cores = lax.axis_size(axis), lax.axis_size("core")

    def hop(steps):
        pairs = [
            (i * cores + c, (i + steps * (1 - 2 * c)) % count * cores + c)
            for i in range(count)
            for c in range(cores)
        ]
        return lax.ppermute(held, (axis, "core"), pairs)

    return jnp.concatenate([hop(n) if n else held for n in NEAR])


def local(
    tokens,
    norm_gain,
    value_proj,
    gate_proj,
    conv_taps,
    recur_map,
    input_map,
    decay_param,
    decay_offset,
    mix_proj,
):
    own_cols, channels = tokens.shape[1], value_proj.shape[1]
    chips, cores, count = (lax.axis_size(name) for name in ("x", "core", "sp"))

    def swap(array):
        return shift(array, "core", 1)

    first, shard = pack_call(value_proj, gate_proj, mix_proj, count)
    weights = exchange(first, "sp")
    held = jnp.stack([tokens, far_hop(tokens, "x")])
    hop_one = far_hop(shard, "sp", -1)
    hop_back = far_hop(shard, "sp")
    mine = near_hops(held, "x")
    gains = [gain.reshape(chips * cores, 1, own_cols) for gain in norm_gain]
    gains[1] = copy_call(gains[1])
    gains[1] = copy_call(gains[1])
    gains[1] = copy_call(gains[1])
    gains[1] = copy_call(gains[1])

    residual = tokens
    for layer in range(LAYERS):
        more = layer + 1 < LAYERS
        if layer:
            mine = exchange(copies[0], "x")
            weights = later_weights
        theirs = swap(mine)
        value_rows, gate_rows, tail = project_call(
            layer == 0, layer > 0, mine, theirs, gains[layer], weights, channels
        )
        before = lax.ppermute(tail, "sp", [(i, i + 1) for i in range(count - 1)])
        cum, state, msg = scan_call(
            layer,
            value_rows,
            before,
            conv_taps,
            decay_param,
            recur_map,
            input_map,
            decay_offset,
            count,
        )
        msgs = exchange(msg, "sp")
        if more:
            _, hop_one = lax.optimization_barrier((msg, hop_one))
            hop_two = far_hop(hop_one, "sp", -1)
        sent = close_call(msgs, cum, state, gate_rows, chips)
        mine = exchange(sent, "x")
        if more:
            held = (shard, hop_back, hop_two, hop_one)
            _, *held = lax.optimization_barrier((sent, *held))
            mix_weights = near_hops(jnp.stack([h[:channels] for h in held]), "sp")
        else:
            mix_weights = weights
        theirs = swap(mine)
        residual, *copies = mix_call(mine, theirs, mix_weights, residual, chips if more else 0)
        if more:
            _, *held = lax.optimization_barrier((copies[0], *held))
            later_weights = near_hops(jnp.stack([h[channels:] for h in held]), "sp")
    return residual


def solution(mesh):
    grid = mesh.devices
    split = Mesh(grid.reshape(*grid.shape[:2], grid.shape[2] // 2, 2), ("grp", "sp", "x", "core"))
    tp = ("x", "core")
    in_specs = (
        P(("grp", "sp"), tp),
        P(),
        P(None, tp, "sp"),
        P(None, tp, "sp"),
        P(None, None, tp),
        P(None, tp, None, None),
        P(None, tp, None, None),
        P(None, tp),
        P(None, tp, "sp"),
        P(None, "sp", tp),
    )
    return jax.shard_map(
        local, mesh=split, in_specs=in_specs, out_specs=P(("grp", "sp"), tp), check_vma=False
    )
```

```python
import functools

import jax
import jax.numpy as jnp
from jax import lax
from jax.experimental import pallas as pl
from jax.experimental.pallas import tpu as pltpu
from jax.sharding import Mesh, PartitionSpec as P


LAYERS = 2
EPS = 1e-06
RATE_SCALE = 8.0
LANES = 128
HALO = 16
NEAR = (-2, -1, 0, 1)


def one_minus_exp(u):
    series = 1.0
    for n in range(9, 1, -1):
        series = 1.0 + u * series * (1.0 / n)
    return jnp.where(u > -0.5, -u * series, 1.0 - jnp.exp(u))


def softplus(x):
    y = jnp.exp(-jnp.abs(x))
    z = y / (2.0 + y)
    series = jnp.zeros_like(z)
    for n in range(17, 0, -2):
        series = series * (z * z) + 1.0 / n
    return jnp.maximum(x, 0.0) + 2.0 * z * series


def scan_kernel(
    layer,
    value_ref,
    before_ref,
    taps_ref,
    param_ref,
    recur_ref,
    input_ref,
    offset_ref,
    cum_ref,
    state_ref,
    msg_ref,
):
    channels, tok = value_ref.shape
    taps = taps_ref.shape[1]
    rate = -RATE_SCALE * softplus(-param_ref[layer : layer + 1, :])
    rest = jnp.zeros((LANES - taps - 1, channels), jnp.float32)
    consts = jnp.concatenate([taps_ref[layer], rate, rest], axis=0)
    consts = jnp.concatenate([consts, jnp.zeros((LANES, LANES - channels), jnp.float32)], axis=1).T
    consts = consts[:channels]
    maps = jnp.concatenate([recur_ref[layer, 0], input_ref[layer, 0]], axis=1)
    value = value_ref[...].astype(jnp.float32)
    full = jnp.concatenate([before_ref[...].astype(jnp.float32), value], axis=1)
    smoothed = consts[:, taps - 1 : taps] * value
    for back in range(1, taps):
        shifted = pltpu.roll(full, back, axis=1)[:, LANES:]
        smoothed = smoothed + consts[:, taps - 1 - back : taps - back] * shifted
    half = smoothed.astype(jnp.bfloat16)
    gates = lax.dot_general(
        maps, half, (((0,), (0,)), ((), ())), preferred_element_type=jnp.float32
    )
    gates = 1.0 / (1.0 + jnp.exp(-gates))
    recur, inputs = gates[:channels], gates[channels:]
    log_decay = consts[:, taps : taps + 1] * recur + offset_ref[layer]
    a = jnp.exp(log_decay)
    b = jnp.sqrt(one_minus_exp(2.0 * log_decay)) * inputs * smoothed
    lane = lax.broadcasted_iota(jnp.int32, (channels, tok), 1)
    step = 1
    while step < tok:
        inside = lane >= step
        b = jnp.where(inside, a * pltpu.roll(b, step, axis=1), 0.0) + b
        a = jnp.where(inside, pltpu.roll(a, step, axis=1), 1.0) * a
        step *= 2
    cum_ref[...] = a
    state_ref[...] = b
    last = jnp.concatenate([a[:, tok - LANES :], b[:, tok - LANES :]], axis=0)
    row = last.T[LANES - 1 : LANES, :]
    msg_ref[...] = jnp.broadcast_to(row[None], msg_ref.shape)


def close_kernel(msgs_ref, cum_ref, state_ref, gate_ref, out_ref):
    channels, tok = cum_ref.shape
    count = msgs_ref.shape[0]
    position = lax.axis_index("sp")
    carry = jnp.zeros((1, channels), jnp.float32)
    for s in range(count - 1):
        line = msgs_ref[s]
        step = line[:, :channels] * carry + line[:, channels:]
        carry = jnp.where(s < position, step, carry)
    wide = jnp.broadcast_to(carry, (LANES, channels)).T
    wide = jnp.concatenate([wide] * (tok // LANES), axis=1)
    hidden = state_ref[...] + cum_ref[...] * wide
    gate = gate_ref[...].astype(jnp.float32)
    branch = (hidden * (gate / (1.0 + jnp.exp(-gate)))).astype(jnp.bfloat16)
    out_ref[...] = jnp.broadcast_to(branch[None], out_ref.shape)


def weight_slot(block, count, hopped):
    if not hopped:
        return block
    steps, far = len(NEAR), count // len(NEAR)
    sign = 1 - 2 * lax.axis_index("core")
    at = lax.rem(sign * (lax.axis_index("sp") - block) + 2 * count - NEAR[0], count)
    return lax.rem(at, steps) * far + lax.rem(sign * lax.div(at, steps) + far, far)


def piece_block(side, slot, chips, slotted):
    core, source = lax.axis_index("core"), slot
    core = core if side == 0 else 1 - core
    if slotted:
        far = chips // len(NEAR)
        behind = slot % far * len(NEAR) + (1 - 2 * core) * NEAR[slot // far]
        source = lax.rem(lax.axis_index("x") + 2 * chips - behind, chips)
    return 2 * source + core


def project_kernel(
    slotted, hopped, mine_ref, theirs_ref, gain_ref, weight_ref, value_ref, gate_ref, edge_ref
):
    chips, held_rows, width = mine_ref.shape
    channels, tok = value_ref.shape
    extra = held_rows - tok
    pieces = (mine_ref, theirs_ref)

    def project(rows_of, count):
        product = jnp.zeros((2 * channels, count), jnp.float32)
        squares = jnp.zeros((count, width), jnp.float32)
        for side in range(2):
            for slot in range(chips):
                block = piece_block(side, slot, chips, slotted)
                held = weight_slot(block, weight_ref.shape[0], hopped)
                wide = rows_of(pieces[side], slot).astype(jnp.float32)
                squares += wide * wide
                scaled = (wide * gain_ref[block]).astype(jnp.bfloat16)
                product += lax.dot_general(
                    weight_ref[held, : 2 * channels, :],
                    scaled,
                    (((1,), (1,)), ((), ())),
                    preferred_element_type=jnp.float32,
                )
        mean = jnp.sum(squares.T, axis=0, keepdims=True) * (1.0 / (2 * chips * width))
        return (product * lax.rsqrt(mean + EPS)).astype(jnp.bfloat16)

    rows = project(lambda ref, slot: ref[slot, extra:, :], tok)
    value_ref[...] = rows[:channels]
    gate_ref[...] = rows[channels:]
    if extra:
        blank = jnp.zeros((LANES - extra, width), jnp.bfloat16)
        edge = project(
            lambda ref, slot: jnp.concatenate([blank, ref[slot, :extra, :]], axis=0), LANES
        )
        edge_ref[...] = edge[:channels]
    else:
        edge_ref[...] = rows[:channels, tok - LANES :]


def mix_kernel(mine_ref, theirs_ref, weight_ref, residual_ref, out_ref, *copies_ref):
    chips, channels, _ = mine_ref.shape
    count, rows, _ = weight_ref.shape
    mixed = residual_ref[...].astype(jnp.float32)
    for slot in range(chips):
        held = [weight_slot(piece_block(side, slot, chips, False), count, True) for side in range(2)]
        branch = jnp.concatenate([mine_ref[slot], theirs_ref[slot]], axis=0)
        weight = jnp.concatenate([weight_ref[at, rows - channels :, :] for at in held], axis=0)
        mixed += lax.dot_general(
            branch, weight, (((0,), (0,)), ((), ())), preferred_element_type=jnp.float32
        )
    mixed = mixed.astype(jnp.bfloat16)
    out_ref[...] = mixed
    for ref in copies_ref:
        ref[...] = jnp.broadcast_to(mixed[None], ref.shape)


def pack_kernel(value_ref, gate_ref, mix_ref, tokens_ref, first_ref, later_ref, last_ref, sems):
    layers, channels, _ = value_ref.shape
    shards = [ref.at[layer] for layer in range(layers) for ref in (value_ref, gate_ref, mix_ref)]
    moves = []
    for k, shard_ref in enumerate(shards):
        rows_ref, at = (first_ref.at[0], k) if k < 2 else (later_ref, k - 2)
        target = rows_ref.at[pl.ds(at * channels, channels)]
        moves.append(pltpu.make_async_copy(shard_ref, target, sems.at[k]))
    last = last_ref.shape[0]
    source = tokens_ref.at[pl.ds(tokens_ref.shape[0] - last, last)]
    moves.append(pltpu.make_async_copy(source, last_ref, sems.at[len(shards)]))
    for move in moves:
        move.start()
    for move in moves:
        move.wait()
    rows = first_ref[0]
    for at in range(1, first_ref.shape[0]):
        first_ref[at] = rows


def vmem(n):
    return [pl.BlockSpec(memory_space=pltpu.VMEM)] * n


def kernel_call(kernel, out_shape, *operands):
    return pl.pallas_call(
        kernel, out_shape=out_shape, in_specs=vmem(len(operands)), out_specs=vmem(len(out_shape))
    )(*(pltpu.with_memory_space_constraint(a, pltpu.VMEM) for a in operands))


def pack_call(value_proj, gate_proj, mix_proj, tokens, count):
    layers, channels, width = value_proj.shape
    dtype = value_proj.dtype
    out = [
        pltpu.VMEM((count, 2 * channels, width), dtype),
        pltpu.VMEM(((3 * layers - 2) * channels, width), dtype),
        pltpu.VMEM((HALO, tokens.shape[1]), tokens.dtype),
    ]
    return pl.pallas_call(
        pack_kernel,
        out_shape=out,
        in_specs=[pl.BlockSpec(memory_space=pl.ANY)] * 4,
        out_specs=vmem(len(out)),
        scratch_shapes=[pltpu.SemaphoreType.DMA((3 * layers + 1,))],
        name="pack",
    )(value_proj, gate_proj, mix_proj, tokens)


def project_call(slotted, hopped, mine, theirs, gains, weights, channels, tok):
    out = [pltpu.VMEM((channels, n), jnp.bfloat16) for n in (tok, tok, LANES)]
    kernel = functools.partial(project_kernel, slotted, hopped)
    return kernel_call(kernel, out, mine, theirs, gains, weights)


def mix_call(mine, theirs, weights, residual, copies):
    shape, dtype = residual.shape, jnp.bfloat16
    if copies:
        out = [pltpu.VMEM(shape, dtype), pltpu.VMEM((copies, *shape), dtype)]
    else:
        out = [jax.ShapeDtypeStruct(shape, dtype)]
    return kernel_call(mix_kernel, out, mine, theirs, weights, residual)


def scan_call(layer, value, before, taps, param, recur_map, input_map, offset, count):
    channels, tok = value.shape
    out = [
        pltpu.VMEM((channels, tok), jnp.float32),
        pltpu.VMEM((channels, tok), jnp.float32),
        pltpu.VMEM((count, 1, 2 * channels), jnp.float32),
    ]
    kernel = functools.partial(scan_kernel, layer)
    operands = (value, before, taps, param, recur_map, input_map, offset)
    return kernel_call(kernel, out, *operands)


def close_call(msgs, cum, state, gate, copies):
    out = [pltpu.VMEM((copies, *cum.shape), jnp.bfloat16)]
    return kernel_call(close_kernel, out, msgs, cum, state, gate)[0]


def copy_kernel(in_ref, out_ref):
    out_ref[...] = in_ref[...]


def copy_call(array):
    return kernel_call(copy_kernel, [pltpu.VMEM(array.shape, array.dtype)], array)[0]


def exchange(copies, axis):
    return lax.all_to_all(copies, axis, split_axis=0, concat_axis=0, tiled=True)


def shift(array, axis, steps):
    count = lax.axis_size(axis)
    return lax.ppermute(array, axis, [(i, (i + steps) % count) for i in range(count)])


def far_hop(array, axis, hops=1):
    return shift(array, axis, len(NEAR) * hops)


def near_hops(held, axis):
    count, cores = lax.axis_size(axis), lax.axis_size("core")

    def hop(steps):
        pairs = [
            (i * cores + c, (i + steps * (1 - 2 * c)) % count * cores + c)
            for i in range(count)
            for c in range(cores)
        ]
        return lax.ppermute(held, (axis, "core"), pairs)

    return jnp.concatenate([hop(n) if n else held for n in NEAR])


def local(
    tokens,
    norm_gain,
    value_proj,
    gate_proj,
    conv_taps,
    recur_map,
    input_map,
    decay_param,
    decay_offset,
    mix_proj,
):
    (tok_rows, own_cols), channels = tokens.shape, value_proj.shape[1]
    chips, cores, count = (lax.axis_size(name) for name in ("x", "core", "sp"))

    def swap(array):
        return shift(array, "core", 1)

    def to_next(array):
        return lax.ppermute(array, "sp", [(i, i + 1) for i in range(count - 1)])

    first, shard, last = pack_call(value_proj, gate_proj, mix_proj, tokens, count)
    last = to_next(last)
    weights = exchange(first, "sp")
    held = jnp.concatenate([last, tokens], axis=0)
    held = jnp.stack([held, far_hop(held, "x")])
    hop_one = far_hop(shard, "sp", -1)
    hop_back = far_hop(shard, "sp")
    mine = near_hops(held, "x")
    gains = [gain.reshape(chips * cores, 1, own_cols) for gain in norm_gain]
    gains[1] = copy_call(gains[1])
    gains[1] = copy_call(gains[1])
    gains[1] = copy_call(gains[1])
    gains[1] = copy_call(gains[1])

    gains[1] = copy_call(gains[1])
    decay_param = copy_call(decay_param)

    residual = tokens
    for layer in range(LAYERS):
        more = layer + 1 < LAYERS
        if layer:
            mine = exchange(copies[0], "x")
            weights = later_weights
        theirs = swap(mine)
        value_rows, gate_rows, edge = project_call(
            layer == 0, layer > 0, mine, theirs, gains[layer], weights, channels, tok_rows
        )
        if layer:
            edge = to_next(edge)
        cum, state, msg = scan_call(
            layer,
            value_rows,
            edge,
            conv_taps,
            decay_param,
            recur_map,
            input_map,
            decay_offset,
            count,
        )
        msgs = exchange(msg, "sp")
        if more:
            _, hop_one = lax.optimization_barrier((msg, hop_one))
            hop_two = far_hop(hop_one, "sp", -1)
        sent = close_call(msgs, cum, state, gate_rows, chips)
        mine = exchange(sent, "x")
        if more:
            held = (shard, hop_back, hop_two, hop_one)
            _, *held = lax.optimization_barrier((sent, *held))
            mix_weights = near_hops(jnp.stack([h[:channels] for h in held]), "sp")
        else:
            mix_weights = weights
        theirs = swap(mine)
        residual, *copies = mix_call(mine, theirs, mix_weights, residual, chips if more else 0)
        if more:
            _, *held = lax.optimization_barrier((copies[0], *held))
            later_weights = near_hops(jnp.stack([h[channels:] for h in held]), "sp")
    return residual


def solution(mesh):
    grid = mesh.devices
    split = Mesh(grid.reshape(*grid.shape[:2], grid.shape[2] // 2, 2), ("grp", "sp", "x", "core"))
    tp = ("x", "core")
    in_specs = (
        P(("grp", "sp"), tp),
        P(),
        P(None, tp, "sp"),
        P(None, tp, "sp"),
        P(None, None, tp),
        P(None, tp, None, None),
        P(None, tp, None, None),
        P(None, tp),
        P(None, tp, "sp"),
        P(None, "sp", tp),
    )
    return jax.shard_map(
        local, mesh=split, in_specs=in_specs, out_specs=P(("grp", "sp"), tp), check_vma=False
    )
```
